32 devices in a mesh: row: 8 (over z, x), col: 4 (over y, core).
Axes of the slice: x: 2, y: 2, z: 4, core: 2. Of those that a mesh axis runs over, the one named last changes fastest.
Arguments:
- tokens: bfloat16 [2, 32768, 2048], P(None, ('row', 'col')), may hold values from -6 to 6
- norm_gain: float32 [2048], replicated, may hold values from 0.1 to 1.9
- mix_weight: bfloat16 [2048, 1024], replicated, may hold values from -0.125 to 0.125
- gate_weight: bfloat16 [2048, 2048], replicated, may hold values from -0.125 to 0.125
- out_weight: bfloat16 [1024, 2048], replicated, may hold values from -0.1875 to 0.1875
Outputs:
- gated: bfloat16 [2, 32768, 2048], P(None, ('row', 'col'))
The draws below stay inside these ranges and needn't reach their ends.
All inputs are finite; a program needn't handle non-finite values.
Results may differ from the reference program's by a relative error of at most 0.017.
Values may be sent and summed in bfloat16 or wider, within the bound.
A program may use at most 128 MiB of HBM per device.

```python
import jax
import jax.numpy as jnp
from jax import lax

D = 2048
GROUPS = 8
GROUP_DIM = 128
FW = 1024
LENGTH = 32768
SEQS = 2


def steps_of(key, dims, split, low, high):
    gain, own = 1.0, jax.random.fold_in(key, 6)
    for dim, shards_of in split:
        steps = jnp.exp(jax.random.uniform(jax.random.fold_in(own, dim), (shards_of,), jnp.float32, low / len(split), high / len(split)))
        gain = gain * jnp.repeat(steps, dims[dim] // shards_of).reshape([-1 if axis == dim else 1 for axis in range(len(dims))])
    return gain


def bell_draw(key, dims, spread, reach, split=(), dtype=jnp.bfloat16):
    loudness = steps_of(key, dims, split, -0.22, 0.18) if split else 1.0
    entries = jax.random.normal(key, dims, jnp.float32) * spread * loudness
    return jnp.minimum(jnp.maximum(entries, -reach), reach).astype(dtype)


def setup_inputs(seed: int = 0) -> dict:
    streams_of = jax.random.split(jax.random.key(seed), 6)
    tokens = bell_draw(streams_of[0], (SEQS, LENGTH, D), 1.0, 6.0, ((1, 32),))
    norm_gain = jnp.clip(1.0 + 0.18 * jax.random.normal(streams_of[1], (D,), jnp.float32), 0.1, 1.9)
    mix_weight = bell_draw(streams_of[2], (D, FW), D ** -0.5, 0.125)
    gate_weight = bell_draw(streams_of[3], (D, D), D ** -0.5, 0.125)
    out_weight = bell_draw(streams_of[4], (FW, D), FW ** -0.5, 0.1875)
    return {"tokens": tokens, "norm_gain": norm_gain, "mix_weight": mix_weight, "gate_weight": gate_weight, "out_weight": out_weight}


def reference(tokens, norm_gain, mix_weight, gate_weight, out_weight):

    def one_sequence(sequence):
        widened = sequence.astype(jnp.float32)
        inverse_rms = lax.rsqrt(lax.optimization_barrier(jnp.mean(widened * widened, axis=-1, keepdims=True)) + 1e-06)
        normed = (widened * inverse_rms * norm_gain.astype(jnp.float32)).astype(jnp.bfloat16)
        mixed_in = jnp.dot(normed, mix_weight, preferred_element_type=jnp.float32).astype(jnp.bfloat16)
        gate_value = jax.nn.sigmoid(jnp.dot(normed, gate_weight, preferred_element_type=jnp.float32))
        grouped = mixed_in.astype(jnp.float32).reshape(LENGTH, GROUPS, GROUP_DIM)
        spectrum = jnp.fft.fft2(grouped, axes=(0, 2), norm='ortho').real
        spectral = spectrum.reshape(LENGTH, GROUPS * GROUP_DIM).astype(jnp.bfloat16)
        mapped = jnp.dot(spectral, out_weight, preferred_element_type=jnp.float32)
        return (gate_value * mapped).astype(jnp.bfloat16)
    return lax.map(one_sequence, tokens)
```

```python
import functools
import math

import jax
import jax.numpy as jnp
import numpy as np
from jax import lax
from jax.experimental import pallas as pl
from jax.experimental.pallas import tpu as pltpu
from jax.sharding import PartitionSpec as P

GROUP_DIM = 128
HALF = GROUP_DIM // 2
BF16 = jnp.bfloat16
F32 = jnp.float32
AXES = ("row", "col")
LANES = 128
BLOCK = 16
WIDE = 256
NT = (((1,), (1,)), ((), ()))
MESH = pl.DeviceIdType.MESH


def angles(left, right, period):
    return (np.outer(left, right) % period) * (2.0 * math.pi / period)


def channel_table():
    phase = angles(np.arange(GROUP_DIM), np.arange(HALF), GROUP_DIM)
    table = np.stack([np.cos(phase), np.sin(phase)], axis=-1)
    table[:, 0, 1] = np.cos(math.pi * np.arange(GROUP_DIM))
    return table.reshape(GROUP_DIM, GROUP_DIM) * GROUP_DIM ** -0.5


def channel_order():
    order = np.zeros((HALF, 2), np.int64)
    order[:, 0] = np.arange(HALF)
    order[:, 1] = GROUP_DIM - np.arange(HALF)
    order[0, 1] = HALF
    pick = np.zeros((GROUP_DIM, GROUP_DIM))
    pick[np.arange(GROUP_DIM), order.reshape(-1)] = 1.0
    return pick


def position_tables(devices, length, first):
    second, fold = length // first, first // devices
    phase = angles(np.arange(first), np.arange(first), first)
    cosine, sine = np.cos(phase), np.sin(phase)
    zero = np.zeros_like(cosine)
    from_left = np.concatenate([cosine, sine, cosine, sine], axis=1)
    from_right = np.concatenate([-sine, cosine, sine, -cosine], axis=1)
    lone_left = np.concatenate([cosine, sine, zero, zero], axis=1)
    lone_right = np.concatenate([zero, zero, cosine, sine], axis=1)

    def interleave(left, right):
        pair = np.stack([left, right]).reshape(2, devices, fold, -1).transpose(0, 2, 1, 3)
        return pair.reshape(2 * first, 4 * first)

    turn = angles(np.arange(second), np.arange(first), length)
    last = angles(np.arange(second), np.arange(second), second)
    closing = np.concatenate([np.cos(last), -np.sin(last)], axis=1) * length ** -0.5
    return (
        interleave(from_left, from_right),
        interleave(lone_left, lone_right),
        np.cos(turn),
        np.sin(turn),
        closing,
    )


def turn_halves(u, cosine, sine, first):
    halves = []
    for half in range(2):
        real = u[..., 2 * half * first : (2 * half + 1) * first]
        imag = u[..., (2 * half + 1) * first : (2 * half + 2) * first]
        halves.append(
            jnp.concatenate(
                [(real * cosine - imag * sine).astype(BF16), (real * sine + imag * cosine).astype(BF16)], axis=-2
            )
        )
    return jnp.concatenate(halves, axis=-1)


def position_transform(x, lone_here, devices, length, first):
    _, channels, here = x.shape
    second, fold = length // first, first // devices
    normal, lone, cosine, sine, closing = position_tables(devices, length, first)
    normal, lone = jnp.asarray(normal, BF16), jnp.asarray(lone, BF16)
    cosine, sine, closing = jnp.asarray(cosine, F32), jnp.asarray(sine, F32), jnp.asarray(closing, BF16)
    g = jnp.stack([jnp.where(lone_here, lone, normal), normal])
    pairs, span = channels // 2, min(first, here)
    x = x.reshape(devices, pairs, 2, fold, second).transpose(1, 2, 3, 0, 4).reshape(pairs, 2 * first, second)
    g = jnp.stack([g[min(pair, 1)] for pair in range(pairs)])
    u = jnp.einsum("pxr,pxj->prj", x, g, preferred_element_type=F32)
    y = jnp.einsum("kx,pxj->pkj", closing, turn_halves(u, cosine, sine, first), preferred_element_type=F32)
    y = y.astype(BF16).reshape(pairs, second, 2, first).transpose(1, 3, 0, 2)
    return y.reshape(devices, here // span, span, channels).transpose(0, 1, 3, 2)


def plain(devices, tokens, norm_gain, mix_weight, gate_weight, out_weight):
    seqs, here, width = tokens.shape
    length = here * devices
    mixed = mix_weight.shape[1]
    groups = mixed // GROUP_DIM
    channels = mixed // devices
    first = max(GROUP_DIM, devices)
    mix = jnp.einsum(
        "dgj,jk->dgk", mix_weight.reshape(width, groups, GROUP_DIM), jnp.asarray(channel_table(), BF16),
        preferred_element_type=F32,
    ).astype(BF16).reshape(width, mixed)
    ordered = jnp.einsum(
        "ij,gjd->gid", jnp.asarray(channel_order(), BF16), out_weight.reshape(groups, GROUP_DIM, width),
        preferred_element_type=F32,
    ).astype(BF16).reshape(mixed, width)
    widened = tokens.astype(F32)
    inverse_rms = lax.rsqrt(jnp.mean(widened * widened, axis=-1, keepdims=True) + 1e-06)
    normed = (widened * inverse_rms * norm_gain).astype(BF16)
    gate_value = jax.nn.sigmoid(jnp.dot(normed, gate_weight, preferred_element_type=F32)).astype(BF16)
    lone_here = lax.axis_index(AXES) * (channels // 2) % HALF == 0

    def exchange(x):
        return lax.all_to_all(x, AXES, split_axis=0, concat_axis=0, tiled=True)

    returned = []
    for seq in range(seqs):
        columns = lax.dot_general(
            mix, normed[seq], (((0,), (1,)), ((), ())), preferred_element_type=F32
        ).astype(BF16).reshape(devices, channels, here)
        returned.append(exchange(position_transform(exchange(columns), lone_here, devices, length, first)))
    spectral = jnp.stack(returned).transpose(0, 2, 4, 1, 3).reshape(seqs, here, mixed)
    mapped = jnp.dot(spectral, ordered, preferred_element_type=F32)
    return (gate_value * mapped).astype(BF16)


def mixer_kernel(
    rows, cols, tokens, gain_in, mix_in, gate_in, out_in, table_in, order_in, eye_in, spread_in, cos_in, sin_in,
    close_in, result, token_v, normed, mix_v, gate_v, out_v, gain_v, table_v, order_v, eye_v, spread_v, cos_v, sin_v,
    close_v, send_f, recv_f, send_r, recv_r, rows_in, rows_out, left_v, stage, load_sem, token_sem, stage_sem,
    send_f_sem, recv_f_sem, send_r_sem, recv_r_sem,
):
    devices = rows * cols
    row, col = lax.axis_index("row"), lax.axis_index("col")
    me = row * cols + col
    parts, tile, width = stage.shape[0], token_v.shape[1], token_v.shape[2]
    tiles = send_f.shape[0]
    seqs = tokens.shape[0]
    per_seq = tiles // seqs
    channels = send_f.shape[2]
    mixed = devices * channels
    first, second = cos_v.shape
    lows = send_r.shape[2]
    per_group = GROUP_DIM // channels

    barrier = pltpu.get_barrier_semaphore()

    def partner(k):
        there_row, there_col = lax.rem(row + lax.rem(k, rows), rows), lax.rem(col + k // rows, cols)
        return there_row, there_col, there_row * cols + there_col

    def greet(k, carry):
        there_row, there_col, _ = partner(k)
        pl.semaphore_signal(barrier, inc=1, device_id=(there_row, there_col), device_id_type=MESH)
        return carry

    def token_load(i):
        slot = lax.rem(i, 2)
        start = pl.multiple_of(lax.rem(i, per_seq) * tile, tile)
        return pltpu.make_async_copy(
            tokens.at[i // per_seq, pl.ds(start, tile), :], token_v.at[slot], token_sem.at[slot]
        )

    loads = [
        pltpu.make_async_copy(here, there, load_sem.at[at])
        for at, (here, there) in enumerate([
            (gain_in, gain_v), (mix_in, mix_v), (table_in, table_v), (spread_in, spread_v), (cos_in, cos_v),
            (sin_in, sin_v), (close_in, close_v), (gate_in, gate_v), (out_in, out_v), (order_in, order_v),
            (eye_in, eye_v),
        ])
    ]
    token_load(0).start()
    for load in loads[:3]:
        load.start()
    lax.fori_loop(1, devices, greet, 0)

    def norm(i):
        slot = lax.rem(i, 2)
        token_load(i).wait()

        def strip(r, carry):
            at = pl.ds(pl.multiple_of(r * 32, 32), 32)
            widened = token_v[slot, at, :].astype(F32)
            inverse_rms = lax.rsqrt(jnp.mean(widened * widened, axis=-1, keepdims=True) + 1e-06)
            normed[i + 1, at, :] = (widened * inverse_rms * gain_v[...]).astype(BF16)
            return carry

        lax.fori_loop(0, tile // 32, strip, 0)

    def send(send_ref, recv_ref, send_sem, recv_sem, i):
        def one(k, carry):
            there_row, there_col, there = partner(k)
            pltpu.make_async_remote_copy(
                src_ref=send_ref.at[i, there], dst_ref=recv_ref.at[i, me], send_sem=send_sem.at[i],
                recv_sem=recv_sem.at[i], device_id=(there_row, there_col), device_id_type=MESH,
            ).start()
            return carry

        recv_ref[i, me] = send_ref[i, me]
        lax.fori_loop(1, devices, one, 0)

    def await_all(ref, sem, i):
        others = ref.at[i, pl.ds(0, devices - 1)]
        pltpu.make_async_copy(others, others, sem.at[i]).wait()

    loads[0].wait()
    norm(0)
    token_load(1).start()
    for load in loads[3:]:
        load.start()
    loads[1].wait()
    loads[2].wait()
    pl.semaphore_wait(barrier, devices - 1)

    def forward(i, carry):
        def columns(n, carry):
            at = pl.ds(pl.multiple_of(n * WIDE, WIDE), WIDE)
            mixed_in = jnp.dot(normed[i + 1], mix_v[:, at], preferred_element_type=F32).astype(BF16)
            for part in range(WIDE // GROUP_DIM):
                turned = lax.dot_general(
                    table_v[...], mixed_in[:, part * GROUP_DIM : (part + 1) * GROUP_DIM], NT,
                    preferred_element_type=F32,
                ).astype(BF16)
                owner = (n * (WIDE // GROUP_DIM) + part) * per_group
                send_f[i, pl.ds(owner, per_group)] = turned.reshape(per_group, channels, tile)
            return carry

        lax.fori_loop(0, mixed // WIDE, columns, 0)
        send(send_f, recv_f, send_f_sem, recv_f_sem, i)

        @pl.when(i + 1 < tiles)
        def _():
            @pl.when(i + 2 < tiles)
            def _():
                token_load(i + 2).start()

            norm(i + 1)

        return carry

    lax.fori_loop(0, tiles, forward, 0)
    for load in loads[3:]:
        load.wait()

    for group in range(mixed // GROUP_DIM):
        at = pl.ds(group * GROUP_DIM, GROUP_DIM)
        out_v[at, :] = jnp.dot(order_v[...], out_v[at, :], preferred_element_type=F32).astype(BF16)

    def transform(seq):
        def block(b, carry):
            these = pl.ds(pl.multiple_of(b * BLOCK, BLOCK), BLOCK)
            for t in range(per_seq):
                for half in range(tile // LANES):
                    rows_in[t * (tile // LANES) + half] = (
                        recv_f[seq * per_seq + t, :, these, half * LANES : (half + 1) * LANES]
                        .astype(F32).reshape(devices * BLOCK, LANES)
                    )
            for pair in range(BLOCK // 2):
                picked = []
                for column in range(2):
                    for t in range(per_seq):
                        at = pl.ds(2 * pair + column, devices, stride=BLOCK)
                        picked.append(
                            jnp.concatenate(
                                [rows_in[t * (tile // LANES) + half, at, :] for half in range(tile // LANES)], axis=1
                            ).astype(BF16)
                        )
                x = jnp.concatenate(picked, axis=0)
                if pair == 0:
                    lone = jnp.logical_and(b == 0, lax.rem(me, per_group) == 0)
                    spread = spread_v[jnp.where(lone, 0, 1)]
                else:
                    spread = spread_v[1]
                u = jnp.dot(spread, x, preferred_element_type=F32)
                cosine, sine = cos_v[...], sin_v[...]
                halves = []
                for half in range(2):
                    real = u[2 * half * first : (2 * half + 1) * first]
                    imag = u[(2 * half + 1) * first : (2 * half + 2) * first]
                    halves.append(
                        jnp.concatenate(
                            [(real * cosine - imag * sine).astype(BF16), (real * sine + imag * cosine).astype(BF16)],
                            axis=1,
                        )
                    )
                turned = jnp.concatenate(halves, axis=0)
                y = lax.dot_general(close_v[...], turned, NT, preferred_element_type=F32)
                for half in range(2):
                    rows_out[pl.ds(2 * pair + half, second, stride=BLOCK), :] = y[:, half * first : (half + 1) * first]

            def leave(there, carry):
                span = second // devices * BLOCK
                out = rows_out[pl.ds(pl.multiple_of(there * span, span), span), :].reshape(-1, BLOCK, LANES)
                for q in range(per_seq):
                    send_r[seq * per_seq + q, there, :, these, :] = out[q * lows : (q + 1) * lows].astype(BF16)
                return carry

            lax.fori_loop(0, devices, leave, 0)
            return carry

        lax.fori_loop(0, channels // BLOCK, block, 0)

    def middle(seq, carry):
        for t in range(per_seq):
            await_all(recv_f, recv_f_sem, seq * per_seq + t)
        transform(seq)
        for q in range(per_seq):
            send(send_r, recv_r, send_r_sem, recv_r_sem, seq * per_seq + q)

        def gate(at, carry):
            i, n = seq * per_seq + at // (width // WIDE), lax.rem(at, width // WIDE)
            these = pl.ds(pl.multiple_of(n * WIDE, WIDE), WIDE)
            logits = jnp.dot(normed[i + 1], gate_v[:, these], preferred_element_type=F32)
            normed[i, :, these] = jax.nn.sigmoid(logits).astype(BF16)
            return carry

        lax.fori_loop(0, per_seq * (width // WIDE), gate, 0)
        return carry

    lax.fori_loop(0, seqs, middle, 0)

    def put(j):
        slot = lax.rem(j, parts)
        start = pl.multiple_of(lax.rem(j, per_seq) * tile, tile)
        return pltpu.make_async_copy(
            stage.at[slot], result.at[j // per_seq, pl.ds(start, tile), :], stage_sem.at[slot]
        )

    def finish(j, carry):
        slot = lax.rem(j, parts)
        await_all(recv_r, recv_r_sem, j)

        @pl.when(j >= parts)
        def _():
            put(j - parts).wait()

        left = jnp.concatenate([recv_r[j, :, low].reshape(mixed, LANES) for low in range(lows)], axis=1)
        left_v[...] = lax.dot_general(eye_v[...], left, NT, preferred_element_type=F32).astype(BF16)

        def columns(n, carry):
            these = pl.ds(pl.multiple_of(n * WIDE, WIDE), WIDE)
            mapped = jnp.dot(left_v[...], out_v[:, these], preferred_element_type=F32)
            stage[slot, :, these] = (normed[j, :, these].astype(F32) * mapped).astype(BF16)
            return carry

        lax.fori_loop(0, width // WIDE, columns, 0)
        put(j).start()
        return carry

    lax.fori_loop(0, tiles, finish, 0)
    for j in range(tiles - parts, tiles):
        put(j).wait()
    for i in range(tiles):
        await_all(send_f, send_f_sem, i)
        await_all(send_r, send_r_sem, i)


def fused(rows, cols, tokens, norm_gain, mix_weight, gate_weight, out_weight):
    devices = rows * cols
    seqs, here, width = tokens.shape
    length = here * devices
    mixed = mix_weight.shape[1]
    channels = mixed // devices
    first = GROUP_DIM
    second = length // first
    tile = second
    tiles = seqs * here // tile
    lows = tile // first
    normal, lone, cosine, sine, closing = position_tables(devices, length, first)
    constants = [
        jnp.asarray(channel_table().T, BF16),
        jnp.asarray(channel_order(), BF16),
        jnp.eye(tile, dtype=BF16),
        jnp.asarray(np.stack([lone.T, normal.T]), BF16),
        jnp.asarray(cosine.T, F32),
        jnp.asarray(sine.T, F32),
        jnp.asarray(closing, BF16),
    ]
    operands = [tokens, norm_gain.reshape(1, width), mix_weight, gate_weight, out_weight, *constants]
    hbm = pl.BlockSpec(memory_space=pl.ANY)
    parts = 2
    scratch = [
        pltpu.VMEM((2, tile, width), BF16),
        pltpu.VMEM((tiles + 1, tile, width), BF16),
        pltpu.VMEM(mix_weight.shape, BF16),
        pltpu.VMEM(gate_weight.shape, BF16),
        pltpu.VMEM(out_weight.shape, BF16),
        pltpu.VMEM((1, width), F32),
        *[pltpu.VMEM(constant.shape, constant.dtype) for constant in constants],
        pltpu.VMEM((tiles, devices, channels, tile), BF16),
        pltpu.VMEM((tiles, devices, channels, tile), BF16),
        pltpu.VMEM((tiles, devices, lows, channels, first), BF16),
        pltpu.VMEM((tiles, devices, lows, channels, first), BF16),
        pltpu.VMEM((here // LANES, devices * BLOCK, LANES), F32),
        pltpu.VMEM((second * BLOCK, first), F32),
        pltpu.VMEM((tile, mixed), BF16),
        pltpu.VMEM((parts, tile, width), BF16),
        pltpu.SemaphoreType.DMA((4 + len(constants),)),
        pltpu.SemaphoreType.DMA((2,)),
        pltpu.SemaphoreType.DMA((parts,)),
        *[pltpu.SemaphoreType.DMA((tiles,)) for _ in range(4)],
    ]
    return pl.pallas_call(
        functools.partial(mixer_kernel, rows, cols),
        in_specs=[hbm] * len(operands),
        out_specs=hbm,
        out_shape=jax.ShapeDtypeStruct(tokens.shape, BF16),
        scratch_shapes=scratch,
        compiler_params=pltpu.CompilerParams(
            collective_id=0, has_side_effects=True, vmem_limit_bytes=60 * 2**20
        ),
        name="mixer",
    )(*operands)


def fits(devices, tokens, mix_weight):
    seqs, here, width = tokens.shape
    mixed = mix_weight.shape[1]
    second = here * devices // GROUP_DIM
    return (
        devices % 16 == 0
        and GROUP_DIM % devices == 0
        and mixed % (devices * BLOCK) == 0
        and second % WIDE == 0
        and here % second == 0
        and here // second == GROUP_DIM // devices
        and mixed % WIDE == 0
        and width % WIDE == 0
    )


def local(rows, cols, tokens, norm_gain, mix_weight, gate_weight, out_weight):
    args = (tokens, norm_gain, mix_weight, gate_weight, out_weight)
    if fits(rows * cols, tokens, mix_weight):
        return fused(rows, cols, *args)
    return plain(rows * cols, *args)


def solution(mesh):
    in_specs = (P(None, AXES, None), P(), P(), P(), P())
    body = functools.partial(local, mesh.shape["row"], mesh.shape["col"])
    return jax.shard_map(body, mesh=mesh, in_specs=in_specs, out_specs=P(None, AXES, None), check_vma=False)
```

```python
import functools
import math

import jax
import jax.numpy as jnp
import numpy as np
from jax import lax
from jax.experimental import pallas as pl
from jax.experimental.pallas import tpu as pltpu
from jax.sharding import PartitionSpec as P

GROUP_DIM = 128
HALF = GROUP_DIM // 2
BF16 = jnp.bfloat16
F32 = jnp.float32
AXES = ("row", "col")
LANES = 128
BLOCK = 16
WIDE = 256
NT = (((1,), (1,)), ((), ()))
MESH = pl.DeviceIdType.MESH


def angles(left, right, period):
    return (np.outer(left, right) % period) * (2.0 * math.pi / period)


def channel_table():
    phase = angles(np.arange(GROUP_DIM), np.arange(HALF), GROUP_DIM)
    table = np.stack([np.cos(phase), np.sin(phase)], axis=-1)
    table[:, 0, 1] = np.cos(math.pi * np.arange(GROUP_DIM))
    return table.reshape(GROUP_DIM, GROUP_DIM) * GROUP_DIM ** -0.5


def channel_order():
    order = np.zeros((HALF, 2), np.int64)
    order[:, 0] = np.arange(HALF)
    order[:, 1] = GROUP_DIM - np.arange(HALF)
    order[0, 1] = HALF
    pick = np.zeros((GROUP_DIM, GROUP_DIM))
    pick[np.arange(GROUP_DIM), order.reshape(-1)] = 1.0
    return pick


def position_tables(devices, length, first):
    second, fold = length // first, first // devices
    phase = angles(np.arange(first), np.arange(first), first)
    cosine, sine = np.cos(phase), np.sin(phase)
    zero = np.zeros_like(cosine)
    from_left = np.concatenate([cosine, sine, cosine, sine], axis=1)
    from_right = np.concatenate([-sine, cosine, sine, -cosine], axis=1)
    lone_left = np.concatenate([cosine, sine, zero, zero], axis=1)
    lone_right = np.concatenate([zero, zero, cosine, sine], axis=1)

    def interleave(left, right):
        pair = np.stack([left, right]).reshape(2, devices, fold, -1).transpose(0, 2, 1, 3)
        return pair.reshape(2 * first, 4 * first)

    turn = angles(np.arange(second), np.arange(first), length)
    last = angles(np.arange(second), np.arange(second), second)
    closing = np.concatenate([np.cos(last), -np.sin(last)], axis=1) * length ** -0.5
    return (
        interleave(from_left, from_right),
        interleave(lone_left, lone_right),
        np.cos(turn),
        np.sin(turn),
        closing,
    )


def turn_halves(u, cosine, sine, first):
    halves = []
    for half in range(2):
        real = u[..., 2 * half * first : (2 * half + 1) * first]
        imag = u[..., (2 * half + 1) * first : (2 * half + 2) * first]
        halves.append(
            jnp.concatenate(
                [(real * cosine - imag * sine).astype(BF16), (real * sine + imag * cosine).astype(BF16)], axis=-2
            )
        )
    return jnp.concatenate(halves, axis=-1)


def position_transform(x, lone_here, devices, length, first):
    _, channels, here = x.shape
    second, fold = length // first, first // devices
    normal, lone, cosine, sine, closing = position_tables(devices, length, first)
    normal, lone = jnp.asarray(normal, BF16), jnp.asarray(lone, BF16)
    cosine, sine, closing = jnp.asarray(cosine, F32), jnp.asarray(sine, F32), jnp.asarray(closing, BF16)
    g = jnp.stack([jnp.where(lone_here, lone, normal), normal])
    pairs, span = channels // 2, min(first, here)
    x = x.reshape(devices, pairs, 2, fold, second).transpose(1, 2, 3, 0, 4).reshape(pairs, 2 * first, second)
    g = jnp.stack([g[min(pair, 1)] for pair in range(pairs)])
    u = jnp.einsum("pxr,pxj->prj", x, g, preferred_element_type=F32)
    y = jnp.einsum("kx,pxj->pkj", closing, turn_halves(u, cosine, sine, first), preferred_element_type=F32)
    y = y.astype(BF16).reshape(pairs, second, 2, first).transpose(1, 3, 0, 2)
    return y.reshape(devices, here // span, span, channels).transpose(0, 1, 3, 2)


def plain(devices, tokens, norm_gain, mix_weight, gate_weight, out_weight):
    seqs, here, width = tokens.shape
    length = here * devices
    mixed = mix_weight.shape[1]
    groups = mixed // GROUP_DIM
    channels = mixed // devices
    first = max(GROUP_DIM, devices)
    mix = jnp.einsum(
        "dgj,jk->dgk", mix_weight.reshape(width, groups, GROUP_DIM), jnp.asarray(channel_table(), BF16),
        preferred_element_type=F32,
    ).astype(BF16).reshape(width, mixed)
    ordered = jnp.einsum(
        "ij,gjd->gid", jnp.asarray(channel_order(), BF16), out_weight.reshape(groups, GROUP_DIM, width),
        preferred_element_type=F32,
    ).astype(BF16).reshape(mixed, width)
    widened = tokens.astype(F32)
    inverse_rms = lax.rsqrt(jnp.mean(widened * widened, axis=-1, keepdims=True) + 1e-06)
    normed = (widened * inverse_rms * norm_gain).astype(BF16)
    gate_value = jax.nn.sigmoid(jnp.dot(normed, gate_weight, preferred_element_type=F32)).astype(BF16)
    lone_here = lax.axis_index(AXES) * (channels // 2) % HALF == 0

    def exchange(x):
        return lax.all_to_all(x, AXES, split_axis=0, concat_axis=0, tiled=True)

    returned = []
    for seq in range(seqs):
        columns = lax.dot_general(
            mix, normed[seq], (((0,), (1,)), ((), ())), preferred_element_type=F32
        ).astype(BF16).reshape(devices, channels, here)
        returned.append(exchange(position_transform(exchange(columns), lone_here, devices, length, first)))
    spectral = jnp.stack(returned).transpose(0, 2, 4, 1, 3).reshape(seqs, here, mixed)
    mapped = jnp.dot(spectral, ordered, preferred_element_type=F32)
    return (gate_value * mapped).astype(BF16)


def mixer_kernel(
    rows, cols, tokens, gain_in, mix_in, gate_in, out_in, table_in, order_in, eye_in, spread_in, cos_in, sin_in,
    close_in, result, token_v, normed, mix_v, gate_v, out_v, gain_v, table_v, order_v, eye_v, spread_v, cos_v, sin_v,
    close_v, send_f, recv_f, send_r, recv_r, rows_in, rows_out, left_v, load_sem, mix_sem, token_sem, send_f_sem, recv_f_sem, send_r_sem, recv_r_sem,
):
    devices = rows * cols
    row, col = lax.axis_index("row"), lax.axis_index("col")
    me = row * cols + col
    tile, width = token_v.shape[1], token_v.shape[2]
    tiles = send_f.shape[0]
    seqs = tokens.shape[0]
    per_seq = tiles // seqs
    channels = send_f.shape[2]
    mixed = devices * channels
    first, second = cos_v.shape
    lows = send_r.shape[2]
    per_group = GROUP_DIM // channels

    barrier = pltpu.get_barrier_semaphore()

    def partner(k):
        there_row, there_col = lax.rem(row + lax.rem(k, rows), rows), lax.rem(col + k // rows, cols)
        return there_row, there_col, there_row * cols + there_col

    def greet(k, carry):
        there_row, there_col, _ = partner(k)
        pl.semaphore_signal(barrier, inc=1, device_id=(there_row, there_col), device_id_type=MESH)
        return carry

    def positions(i):
        return pl.ds(pl.multiple_of(lax.rem(i, per_seq) * tile, tile), tile)

    def token_load(i):
        slot = lax.rem(i, 2)
        return pltpu.make_async_copy(
            tokens.at[i // per_seq, positions(i), :], token_v.at[slot], token_sem.at[slot]
        )

    span = WIDE // channels
    chunks = devices // span
    mine, within = me // span, lax.rem(me, span)

    def chunk_at(step):
        shift = jnp.where(step == 0, chunks // 2, step + jnp.where(step >= chunks // 2, 1, 0))
        return lax.rem(mine + shift, chunks)

    def wide(n):
        return pl.ds(pl.multiple_of(n * WIDE, WIDE), WIDE)

    def mix_load(step):
        these = wide(chunk_at(step))
        return pltpu.make_async_copy(mix_in.at[:, these], mix_v.at[:, these], mix_sem.at[step])

    loads = [
        pltpu.make_async_copy(here, there, load_sem.at[at])
        for at, (here, there) in enumerate([
            (gain_in, gain_v), (table_in, table_v), (spread_in, spread_v), (cos_in, cos_v), (sin_in, sin_v),
            (close_in, close_v), (gate_in, gate_v), (out_in, out_v), (order_in, order_v), (eye_in, eye_v),
        ])
    ]
    token_load(0).start()
    loads[0].start()
    loads[1].start()
    for step in range(chunks):
        mix_load(step).start()
    token_load(1).start()
    lax.fori_loop(1, devices, greet, 0)

    def norm(i):
        slot = lax.rem(i, 2)
        token_load(i).wait()

        def strip(r, carry):
            at = pl.ds(pl.multiple_of(r * 32, 32), 32)
            widened = token_v[slot, at, :].astype(F32)
            inverse_rms = lax.rsqrt(jnp.mean(widened * widened, axis=-1, keepdims=True) + 1e-06)
            normed[i, at, :] = (widened * inverse_rms * gain_v[...]).astype(BF16)
            return carry

        lax.fori_loop(0, tile // 32, strip, 0)

    def send_chunk(send_ref, recv_ref, send_sem, recv_sem, i, chunk):
        def one(k, carry):
            there = chunk * span + lax.rem(within + k, span)
            there_row, there_col = there // cols, lax.rem(there, cols)

            @pl.when(there != me)
            def _():
                pltpu.make_async_remote_copy(
                    src_ref=send_ref.at[i, there], dst_ref=recv_ref.at[i, me], send_sem=send_sem.at[i],
                    recv_sem=recv_sem.at[i], device_id=(there_row, there_col), device_id_type=MESH,
                ).start()

            return carry

        lax.fori_loop(0, span, one, 0)

    def send(send_ref, recv_ref, send_sem, recv_sem, i):
        def one(step, carry):
            send_chunk(send_ref, recv_ref, send_sem, recv_sem, i, chunk_at(step))
            return carry

        recv_ref[i, me] = send_ref[i, me]
        lax.fori_loop(0, chunks, one, 0)

    def await_all(ref, sem, i):
        others = ref.at[i, pl.ds(0, devices - 1)]
        pltpu.make_async_copy(others, others, sem.at[i]).wait()

    def compute(m):
        i, step = m // chunks, lax.rem(m, chunks)

        @pl.when(step == 0)
        def _():
            norm(i)

            @pl.when(i + 2 < tiles)
            def _():
                token_load(i + 2).start()

        @pl.when(i == 0)
        def _():
            mix_load(step).wait()

        n = chunk_at(step)
        mixed_in = jnp.dot(normed[i], mix_v[:, wide(n)], preferred_element_type=F32).astype(BF16)
        for part in range(WIDE // GROUP_DIM):
            turned = lax.dot_general(
                table_v[...], mixed_in[:, part * GROUP_DIM : (part + 1) * GROUP_DIM], NT,
                preferred_element_type=F32,
            ).astype(BF16)
            send_f[i, pl.ds(n * span + part * per_group, per_group)] = turned.reshape(per_group, channels, tile)

    def forward(m, carry):
        i, step = m // chunks, lax.rem(m, chunks)
        n = chunk_at(step)

        @pl.when(n == mine)
        def _():
            recv_f[i, me] = send_f[i, me]

        send_chunk(send_f, recv_f, send_f_sem, recv_f_sem, i, n)

        @pl.when(m + 1 < tiles * chunks)
        def _():
            compute(m + 1)

        return carry

    loads[0].wait()
    loads[1].wait()
    compute(0)
    for load in loads[2:]:
        load.start()
    pl.semaphore_wait(barrier, devices - 1)
    lax.fori_loop(0, tiles * chunks, forward, 0)
    for load in loads[2:]:
        load.wait()

    for group in range(mixed // GROUP_DIM):
        at = pl.ds(group * GROUP_DIM, GROUP_DIM)
        out_v[at, :] = jnp.dot(order_v[...], out_v[at, :], preferred_element_type=F32).astype(BF16)

    def transform(seq):
        def block(b, carry):
            these = pl.ds(pl.multiple_of(b * BLOCK, BLOCK), BLOCK)
            for t in range(per_seq):
                for half in range(tile // LANES):
                    rows_in[t * (tile // LANES) + half] = (
                        recv_f[seq * per_seq + t, :, these, half * LANES : (half + 1) * LANES]
                        .astype(F32).reshape(devices * BLOCK, LANES)
                    )
            for pair in range(BLOCK // 2):
                picked = []
                for column in range(2):
                    for t in range(per_seq):
                        at = pl.ds(2 * pair + column, devices, stride=BLOCK)
                        picked.append(
                            jnp.concatenate(
                                [rows_in[t * (tile // LANES) + half, at, :] for half in range(tile // LANES)], axis=1
                            ).astype(BF16)
                        )
                x = jnp.concatenate(picked, axis=0)
                if pair == 0:
                    lone = jnp.logical_and(b == 0, lax.rem(me, per_group) == 0)
                    spread = spread_v[jnp.where(lone, 0, 1)]
                else:
                    spread = spread_v[1]
                u = jnp.dot(spread, x, preferred_element_type=F32)
                cosine, sine = cos_v[...], sin_v[...]
                halves = []
                for half in range(2):
                    real = u[2 * half * first : (2 * half + 1) * first]
                    imag = u[(2 * half + 1) * first : (2 * half + 2) * first]
                    halves.append(
                        jnp.concatenate(
                            [(real * cosine - imag * sine).astype(BF16), (real * sine + imag * cosine).astype(BF16)],
                            axis=1,
                        )
                    )
                turned = jnp.concatenate(halves, axis=0)
                y = lax.dot_general(close_v[...], turned, NT, preferred_element_type=F32)
                for half in range(2):
                    rows_out[pl.ds(2 * pair + half, second, stride=BLOCK), :] = y[:, half * first : (half + 1) * first]

            def leave(there, carry):
                span = second // devices * BLOCK
                out = rows_out[pl.ds(pl.multiple_of(there * span, span), span), :].reshape(-1, BLOCK, LANES)
                for q in range(per_seq):
                    send_r[seq * per_seq + q, there, :, these, :] = out[q * lows : (q + 1) * lows].astype(BF16)
                return carry

            lax.fori_loop(0, devices, leave, 0)
            return carry

        lax.fori_loop(0, channels // BLOCK, block, 0)

    def middle(seq, carry):
        for t in range(per_seq):
            await_all(recv_f, recv_f_sem, seq * per_seq + t)
        transform(seq)
        for q in range(per_seq):
            send(send_r, recv_r, send_r_sem, recv_r_sem, seq * per_seq + q)

        def gate(at, carry):
            i, n = seq * per_seq + at // (width // WIDE), lax.rem(at, width // WIDE)
            these = wide(n)
            logits = jnp.dot(normed[i], gate_v[:, these], preferred_element_type=F32)
            result[seq, positions(i), these] = jax.nn.sigmoid(logits).astype(BF16)
            return carry

        lax.fori_loop(0, per_seq * (width // WIDE), gate, 0)
        return carry

    lax.fori_loop(0, seqs, middle, 0)

    def finish(j, carry):
        await_all(recv_r, recv_r_sem, j)
        left = jnp.concatenate([recv_r[j, :, low].reshape(mixed, LANES) for low in range(lows)], axis=1)
        left_v[...] = lax.dot_general(eye_v[...], left, NT, preferred_element_type=F32).astype(BF16)

        def columns(n, carry):
            these = wide(n)
            mapped = jnp.dot(left_v[...], out_v[:, these], preferred_element_type=F32)
            at = (j // per_seq, positions(j), these)
            result[at] = (result[at].astype(F32) * mapped).astype(BF16)
            return carry

        lax.fori_loop(0, width // WIDE, columns, 0)
        return carry

    lax.fori_loop(0, tiles, finish, 0)
    for i in range(tiles):
        await_all(send_f, send_f_sem, i)
        await_all(send_r, send_r_sem, i)


def fused(rows, cols, tokens, norm_gain, mix_weight, gate_weight, out_weight):
    devices = rows * cols
    seqs, here, width = tokens.shape
    length = here * devices
    mixed = mix_weight.shape[1]
    channels = mixed // devices
    first = GROUP_DIM
    second = length // first
    tile = second
    tiles = seqs * here // tile
    lows = tile // first
    normal, lone, cosine, sine, closing = position_tables(devices, length, first)
    constants = [
        jnp.asarray(channel_table().T, BF16),
        jnp.asarray(channel_order(), BF16),
        jnp.asarray(np.eye(tile), BF16),
        jnp.asarray(np.stack([lone.T, normal.T]), BF16),
        jnp.asarray(cosine.T, F32),
        jnp.asarray(sine.T, F32),
        jnp.asarray(closing, BF16),
    ]
    operands = [tokens, norm_gain.reshape(1, width), mix_weight, gate_weight, out_weight, *constants]
    hbm = pl.BlockSpec(memory_space=pl.ANY)
    scratch = [
        pltpu.VMEM((2, tile, width), BF16),
        pltpu.VMEM((tiles, tile, width), BF16),
        pltpu.VMEM(mix_weight.shape, BF16),
        pltpu.VMEM(gate_weight.shape, BF16),
        pltpu.VMEM(out_weight.shape, BF16),
        pltpu.VMEM((1, width), F32),
        *[pltpu.VMEM(constant.shape, constant.dtype) for constant in constants],
        pltpu.VMEM((tiles, devices, channels, tile), BF16),
        pltpu.VMEM((tiles, devices, channels, tile), BF16),
        pltpu.VMEM((tiles, devices, lows, channels, first), BF16),
        pltpu.VMEM((tiles, devices, lows, channels, first), BF16),
        pltpu.VMEM((here // LANES, devices * BLOCK, LANES), F32),
        pltpu.VMEM((second * BLOCK, first), F32),
        pltpu.VMEM((tile, mixed), BF16),
        pltpu.SemaphoreType.DMA((3 + len(constants),)),
        pltpu.SemaphoreType.DMA((mixed // WIDE,)),
        pltpu.SemaphoreType.DMA((2,)),
        *[pltpu.SemaphoreType.DMA((tiles,)) for _ in range(4)],
    ]
    return pl.pallas_call(
        functools.partial(mixer_kernel, rows, cols),
        in_specs=[hbm] * len(operands),
        out_specs=pl.BlockSpec(memory_space=pltpu.VMEM),
        out_shape=pltpu.VMEM(tokens.shape, BF16),
        scratch_shapes=scratch,
        compiler_params=pltpu.CompilerParams(
            collective_id=0, has_side_effects=True, vmem_limit_bytes=54 * 2**20
        ),
        name="mixer",
    )(*operands)


def fits(devices, tokens, mix_weight):
    seqs, here, width = tokens.shape
    mixed = mix_weight.shape[1]
    second = here * devices // GROUP_DIM
    return (
        devices % 16 == 0
        and GROUP_DIM % devices == 0
        and mixed % (devices * BLOCK) == 0
        and second % WIDE == 0
        and here % second == 0
        and here // second == GROUP_DIM // devices
        and mixed % WIDE == 0
        and width % WIDE == 0
    )


def local(rows, cols, tokens, norm_gain, mix_weight, gate_weight, out_weight):
    args = (tokens, norm_gain, mix_weight, gate_weight, out_weight)
    if fits(rows * cols, tokens, mix_weight):
        return fused(rows, cols, *args)
    return plain(rows * cols, *args)


def solution(mesh):
    in_specs = (P(None, AXES, None), P(), P(), P(), P())
    body = functools.partial(local, mesh.shape["row"], mesh.shape["col"])
    return jax.shard_map(body, mesh=mesh, in_specs=in_specs, out_specs=P(None, AXES, None), check_vma=False)
```

```python
import functools
import math

import jax
import jax.numpy as jnp
import numpy as np
from jax import lax
from jax.experimental import pallas as pl
from jax.experimental.pallas import tpu as pltpu
from jax.sharding import PartitionSpec as P

GROUP_DIM = 128
HALF = GROUP_DIM // 2
BF16 = jnp.bfloat16
F32 = jnp.float32
AXES = ("row", "col")
LANES = 128
BLOCK = 16
WIDE = 256
NT = (((1,), (1,)), ((), ()))
MESH = pl.DeviceIdType.MESH


def angles(left, right, period):
    return (np.outer(left, right) % period) * (2.0 * math.pi / period)


def channel_table():
    phase = angles(np.arange(GROUP_DIM), np.arange(HALF), GROUP_DIM)
    table = np.stack([np.cos(phase), np.sin(phase)], axis=-1)
    table[:, 0, 1] = np.cos(math.pi * np.arange(GROUP_DIM))
    return table.reshape(GROUP_DIM, GROUP_DIM) * GROUP_DIM ** -0.5


def channel_order():
    order = np.zeros((HALF, 2), np.int64)
    order[:, 0] = np.arange(HALF)
    order[:, 1] = GROUP_DIM - np.arange(HALF)
    order[0, 1] = HALF
    pick = np.zeros((GROUP_DIM, GROUP_DIM))
    pick[np.arange(GROUP_DIM), order.reshape(-1)] = 1.0
    return pick


def position_tables(devices, length, first):
    second, fold = length // first, first // devices
    phase = angles(np.arange(first), np.arange(first), first)
    cosine, sine = np.cos(phase), np.sin(phase)
    zero = np.zeros_like(cosine)
    from_left = np.concatenate([cosine, sine, cosine, sine], axis=1)
    from_right = np.concatenate([-sine, cosine, sine, -cosine], axis=1)
    lone_left = np.concatenate([cosine, sine, zero, zero], axis=1)
    lone_right = np.concatenate([zero, zero, cosine, sine], axis=1)

    def interleave(left, right):
        pair = np.stack([left, right]).reshape(2, devices, fold, -1).transpose(0, 2, 1, 3)
        return pair.reshape(2 * first, 4 * first)

    turn = angles(np.arange(second), np.arange(first), length)
    last = angles(np.arange(second), np.arange(second), second)
    closing = np.concatenate([np.cos(last), -np.sin(last)], axis=1) * length ** -0.5
    return (
        interleave(from_left, from_right),
        interleave(lone_left, lone_right),
        np.cos(turn),
        np.sin(turn),
        closing,
    )


def turn_halves(u, cosine, sine, first):
    halves = []
    for half in range(2):
        real = u[..., 2 * half * first : (2 * half + 1) * first]
        imag = u[..., (2 * half + 1) * first : (2 * half + 2) * first]
        halves.append(
            jnp.concatenate(
                [(real * cosine - imag * sine).astype(BF16), (real * sine + imag * cosine).astype(BF16)], axis=-2
            )
        )
    return jnp.concatenate(halves, axis=-1)


def position_transform(x, lone_here, devices, length, first):
    _, channels, here = x.shape
    second, fold = length // first, first // devices
    normal, lone, cosine, sine, closing = position_tables(devices, length, first)
    normal, lone = jnp.asarray(normal, BF16), jnp.asarray(lone, BF16)
    cosine, sine, closing = jnp.asarray(cosine, F32), jnp.asarray(sine, F32), jnp.asarray(closing, BF16)
    g = jnp.stack([jnp.where(lone_here, lone, normal), normal])
    pairs, span = channels // 2, min(first, here)
    x = x.reshape(devices, pairs, 2, fold, second).transpose(1, 2, 3, 0, 4).reshape(pairs, 2 * first, second)
    g = jnp.stack([g[min(pair, 1)] for pair in range(pairs)])
    u = jnp.einsum("pxr,pxj->prj", x, g, preferred_element_type=F32)
    y = jnp.einsum("kx,pxj->pkj", closing, turn_halves(u, cosine, sine, first), preferred_element_type=F32)
    y = y.astype(BF16).reshape(pairs, second, 2, first).transpose(1, 3, 0, 2)
    return y.reshape(devices, here // span, span, channels).transpose(0, 1, 3, 2)


def plain(devices, tokens, norm_gain, mix_weight, gate_weight, out_weight):
    seqs, here, width = tokens.shape
    length = here * devices
    mixed = mix_weight.shape[1]
    groups = mixed // GROUP_DIM
    channels = mixed // devices
    first = max(GROUP_DIM, devices)
    mix = jnp.einsum(
        "dgj,jk->dgk", mix_weight.reshape(width, groups, GROUP_DIM), jnp.asarray(channel_table(), BF16),
        preferred_element_type=F32,
    ).astype(BF16).reshape(width, mixed)
    ordered = jnp.einsum(
        "ij,gjd->gid", jnp.asarray(channel_order(), BF16), out_weight.reshape(groups, GROUP_DIM, width),
        preferred_element_type=F32,
    ).astype(BF16).reshape(mixed, width)
    widened = tokens.astype(F32)
    inverse_rms = lax.rsqrt(jnp.mean(widened * widened, axis=-1, keepdims=True) + 1e-06)
    normed = (widened * inverse_rms * norm_gain).astype(BF16)
    gate_value = jax.nn.sigmoid(jnp.dot(normed, gate_weight, preferred_element_type=F32)).astype(BF16)
    lone_here = lax.axis_index(AXES) * (channels // 2) % HALF == 0

    def exchange(x):
        return lax.all_to_all(x, AXES, split_axis=0, concat_axis=0, tiled=True)

    returned = []
    for seq in range(seqs):
        columns = lax.dot_general(
            mix, normed[seq], (((0,), (1,)), ((), ())), preferred_element_type=F32
        ).astype(BF16).reshape(devices, channels, here)
        returned.append(exchange(position_transform(exchange(columns), lone_here, devices, length, first)))
    spectral = jnp.stack(returned).transpose(0, 2, 4, 1, 3).reshape(seqs, here, mixed)
    mapped = jnp.dot(spectral, ordered, preferred_element_type=F32)
    return (gate_value * mapped).astype(BF16)


def mixer_kernel(
    rows, cols, tokens, gain_in, mix_in, gate_in, out_in, table_in, order_in, eye_in, spread_in, cos_in, sin_in,
    close_in, result, left_v, out_v, token_v, normed, mix_v, gate_v, gain_v, table_v, order_v, eye_v, spread_v, cos_v,
    sin_v, close_v, send_f, recv_f, send_r, recv_r, rows_in, rows_out, load_sem, mix_sem, token_sem, send_f_sem, recv_f_sem, send_r_sem, recv_r_sem,
):
    devices = rows * cols
    row, col = lax.axis_index("row"), lax.axis_index("col")
    me = row * cols + col
    tile, width = token_v.shape[1], token_v.shape[2]
    tiles = send_f.shape[0]
    seqs = tokens.shape[0]
    per_seq = tiles // seqs
    channels = send_f.shape[2]
    mixed = devices * channels
    first, second = cos_v.shape
    lows = send_r.shape[2]
    per_group = GROUP_DIM // channels

    barrier = pltpu.get_barrier_semaphore()

    span = WIDE // channels
    chunks = devices // span
    mine, within = me // span, lax.rem(me, span)

    def partner(chunk, k):
        there = chunk * span + lax.rem(within + k, span)
        return there, (there // cols, lax.rem(there, cols))

    for shift in range(chunks):
        far = lax.rem(2 * chunks - 1 - mine + shift, chunks)
        for k in range(span):
            there, address = partner(far, k)

            @pl.when(there != me)
            def _():
                pl.semaphore_signal(barrier, inc=1, device_id=address, device_id_type=MESH)

    def positions(i):
        return pl.ds(pl.multiple_of(lax.rem(i, per_seq) * tile, tile), tile)

    def token_load(i):
        slot = lax.rem(i, 2)
        return pltpu.make_async_copy(
            tokens.at[i // per_seq, positions(i), :], token_v.at[slot], token_sem.at[slot]
        )

    def chunk_at(step):
        shift = jnp.where(step == 0, chunks // 2, step + jnp.where(step >= chunks // 2, 1, 0))
        return lax.rem(mine + shift, chunks)

    def wide(n):
        return pl.ds(pl.multiple_of(n * WIDE, WIDE), WIDE)

    def mix_load(step):
        these = wide(chunk_at(step))
        return pltpu.make_async_copy(mix_in.at[:, these], mix_v.at[:, these], mix_sem.at[step])

    loads = [
        pltpu.make_async_copy(here, there, load_sem.at[at])
        for at, (here, there) in enumerate([
            (gain_in, gain_v), (table_in, table_v), (spread_in, spread_v), (cos_in, cos_v), (sin_in, sin_v),
            (close_in, close_v), (gate_in, gate_v), (out_in, out_v), (order_in, order_v), (eye_in, eye_v),
        ])
    ]
    token_load(0).start()
    loads[0].start()
    loads[1].start()
    for step in range(chunks):
        mix_load(step).start()
    token_load(1).start()

    def norm(i):
        slot = lax.rem(i, 2)
        token_load(i).wait()

        def strip(r, carry):
            at = pl.ds(pl.multiple_of(r * 32, 32), 32)
            widened = token_v[slot, at, :].astype(F32)
            inverse_rms = lax.rsqrt(jnp.mean(widened * widened, axis=-1, keepdims=True) + 1e-06)
            normed[i, at, :] = (widened * inverse_rms * gain_v[...]).astype(BF16)
            return carry

        lax.fori_loop(0, tile // 32, strip, 0)

    def send_chunk(send_ref, recv_ref, send_sem, recv_sem, i, chunk):
        def one(k, carry):
            there, address = partner(chunk, k)

            @pl.when(there != me)
            def _():
                pltpu.make_async_remote_copy(
                    src_ref=send_ref.at[i, there], dst_ref=recv_ref.at[i, me], send_sem=send_sem.at[i],
                    recv_sem=recv_sem.at[i], device_id=address, device_id_type=MESH,
                ).start()

            return carry

        lax.fori_loop(0, span, one, 0)

    def send(send_ref, recv_ref, send_sem, recv_sem, i):
        def one(step, carry):
            send_chunk(send_ref, recv_ref, send_sem, recv_sem, i, chunk_at(step))
            return carry

        recv_ref[i, me] = send_ref[i, me]
        lax.fori_loop(0, chunks, one, 0)

    def await_all(ref, sem, i):
        others = ref.at[i, pl.ds(0, devices - 1)]
        pltpu.make_async_copy(others, others, sem.at[i]).wait()

    def compute(m):
        i, step = m // chunks, lax.rem(m, chunks)

        @pl.when(step == 0)
        def _():
            norm(i)

            @pl.when(i + 2 < tiles)
            def _():
                token_load(i + 2).start()

        @pl.when(i == 0)
        def _():
            mix_load(step).wait()

        n = chunk_at(step)
        mixed_in = jnp.dot(normed[i], mix_v[:, wide(n)], preferred_element_type=F32).astype(BF16)
        for part in range(WIDE // GROUP_DIM):
            turned = lax.dot_general(
                table_v[...], mixed_in[:, part * GROUP_DIM : (part + 1) * GROUP_DIM], NT,
                preferred_element_type=F32,
            ).astype(BF16)
            send_f[i, pl.ds(n * span + part * per_group, per_group)] = turned.reshape(per_group, channels, tile)

    def post(m):
        i, n = m // chunks, chunk_at(lax.rem(m, chunks))

        @pl.when(n == mine)
        def _():
            recv_f[i, me] = send_f[i, me]

        send_chunk(send_f, recv_f, send_f_sem, recv_f_sem, i, n)

    def forward(m, carry):
        compute(m + 1)

        @pl.when(m > 0)
        def _():
            post(m)

        return carry

    pieces = tiles * chunks
    loads[0].wait()
    loads[1].wait()
    compute(0)
    for load in loads[2:]:
        load.start()
    pl.semaphore_wait(barrier, devices - 1)
    post(0)
    lax.fori_loop(0, pieces - 1, forward, 0)
    for load in loads[2:]:
        load.wait()
    post(pieces - 1)

    for group in range(mixed // GROUP_DIM):
        at = pl.ds(group * GROUP_DIM, GROUP_DIM)
        out_v[at, :] = jnp.dot(order_v[...], out_v[at, :], preferred_element_type=F32).astype(BF16)

    def transform(seq):
        def block(b, carry):
            these = pl.ds(pl.multiple_of(b * BLOCK, BLOCK), BLOCK)
            for t in range(per_seq):
                for half in range(tile // LANES):
                    rows_in[t * (tile // LANES) + half] = (
                        recv_f[seq * per_seq + t, :, these, half * LANES : (half + 1) * LANES]
                        .astype(F32).reshape(devices * BLOCK, LANES)
                    )
            for pair in range(BLOCK // 2):
                picked = []
                for column in range(2):
                    for t in range(per_seq):
                        at = pl.ds(2 * pair + column, devices, stride=BLOCK)
                        picked.append(
                            jnp.concatenate(
                                [rows_in[t * (tile // LANES) + half, at, :] for half in range(tile // LANES)], axis=1
                            ).astype(BF16)
                        )
                x = jnp.concatenate(picked, axis=0)
                if pair == 0:
                    lone = jnp.logical_and(b == 0, lax.rem(me, per_group) == 0)
                    spread = spread_v[jnp.where(lone, 0, 1)]
                else:
                    spread = spread_v[1]
                u = jnp.dot(spread, x, preferred_element_type=F32)
                cosine, sine = cos_v[...], sin_v[...]
                halves = []
                for half in range(2):
                    real = u[2 * half * first : (2 * half + 1) * first]
                    imag = u[(2 * half + 1) * first : (2 * half + 2) * first]
                    halves.append(
                        jnp.concatenate(
                            [(real * cosine - imag * sine).astype(BF16), (real * sine + imag * cosine).astype(BF16)],
                            axis=1,
                        )
                    )
                turned = jnp.concatenate(halves, axis=0)
                y = lax.dot_general(close_v[...], turned, NT, preferred_element_type=F32)
                for half in range(2):
                    rows_out[pl.ds(2 * pair + half, second, stride=BLOCK), :] = y[:, half * first : (half + 1) * first]

            def leave(there, carry):
                span = second // devices * BLOCK
                out = rows_out[pl.ds(pl.multiple_of(there * span, span), span), :].reshape(-1, BLOCK, LANES)
                for q in range(per_seq):
                    send_r[seq * per_seq + q, there, :, these, :] = out[q * lows : (q + 1) * lows].astype(BF16)
                return carry

            lax.fori_loop(0, devices, leave, 0)
            return carry

        lax.fori_loop(0, channels // BLOCK, block, 0)

    def middle(seq, carry):
        for t in range(per_seq):
            await_all(recv_f, recv_f_sem, seq * per_seq + t)
        transform(seq)
        def gate(at, carry):
            i, n = seq * per_seq + at // (width // WIDE), lax.rem(at, width // WIDE)
            these = wide(n)
            logits = jnp.dot(normed[i], gate_v[:, these], preferred_element_type=F32)
            result[seq, positions(i), these] = jax.nn.sigmoid(logits).astype(BF16)
            return carry

        lax.fori_loop(0, per_seq * (width // WIDE), gate, 0)
        for q in range(per_seq):
            send(send_r, recv_r, send_r_sem, recv_r_sem, seq * per_seq + q)
        return carry

    lax.fori_loop(0, seqs, middle, 0)

    def gather(j):
        await_all(recv_r, recv_r_sem, j)
        left = jnp.concatenate([recv_r[j, :, low].reshape(mixed, LANES) for low in range(lows)], axis=1)
        left_v[...] = lax.dot_general(eye_v[...], left, NT, preferred_element_type=F32).astype(BF16)

    def finish(j, carry):
        gather(j)

        def columns(n, carry):
            at = (j // per_seq, positions(j), wide(n))
            mapped = jnp.dot(left_v[...], out_v[:, wide(n)], preferred_element_type=F32)
            result[at] = (result[at].astype(F32) * mapped).astype(BF16)
            return carry

        lax.fori_loop(0, width // WIDE, columns, 0)
        return carry

    lax.fori_loop(0, tiles - 1, finish, 0)
    gather(tiles - 1)
    for i in range(tiles):
        await_all(send_f, send_f_sem, i)
        await_all(send_r, send_r_sem, i)


def last_kernel(gated, left, out_v, final, stage, sems):
    tile, width = stage.shape
    per_seq = gated.shape[1] // tile
    tiles = sems.shape[0]

    def put(j):
        at = (j // per_seq, pl.ds(j % per_seq * tile, tile))
        return pltpu.make_async_copy(gated.at[at] if j + 1 < tiles else stage, final.at[at], sems.at[j])

    for j in range(tiles - 1):
        put(j).start()

    def columns(n, carry):
        at = pl.ds(pl.multiple_of(n * WIDE, WIDE), WIDE)
        mapped = jnp.dot(left[...], out_v[:, at], preferred_element_type=F32)
        gate = gated[gated.shape[0] - 1, gated.shape[1] - tile :, at].astype(F32)
        stage[:, at] = (gate * mapped).astype(BF16)
        return carry

    lax.fori_loop(0, width // WIDE, columns, 0)
    put(tiles - 1).start()
    for j in range(tiles):
        put(j).wait()


def fused(rows, cols, tokens, norm_gain, mix_weight, gate_weight, out_weight):
    devices = rows * cols
    seqs, here, width = tokens.shape
    length = here * devices
    mixed = mix_weight.shape[1]
    channels = mixed // devices
    first = GROUP_DIM
    second = length // first
    tile = second
    tiles = seqs * here // tile
    lows = tile // first
    normal, lone, cosine, sine, closing = position_tables(devices, length, first)
    constants = [
        jnp.asarray(channel_table().T, BF16),
        jnp.asarray(channel_order(), BF16),
        jnp.asarray(np.eye(tile), BF16),
        jnp.asarray(np.stack([lone.T, normal.T]), BF16),
        jnp.asarray(cosine.T, F32),
        jnp.asarray(sine.T, F32),
        jnp.asarray(closing, BF16),
    ]
    operands = [tokens, norm_gain.reshape(1, width), mix_weight, gate_weight, out_weight, *constants]
    hbm = pl.BlockSpec(memory_space=pl.ANY)
    scratch = [
        pltpu.VMEM((2, tile, width), BF16),
        pltpu.VMEM((tiles, tile, width), BF16),
        pltpu.VMEM(mix_weight.shape, BF16),
        pltpu.VMEM(gate_weight.shape, BF16),
        pltpu.VMEM((1, width), F32),
        *[pltpu.VMEM(constant.shape, constant.dtype) for constant in constants],
        pltpu.VMEM((tiles, devices, channels, tile), BF16),
        pltpu.VMEM((tiles, devices, channels, tile), BF16),
        pltpu.VMEM((tiles, devices, lows, channels, first), BF16),
        pltpu.VMEM((tiles, devices, lows, channels, first), BF16),
        pltpu.VMEM((here // LANES, devices * BLOCK, LANES), F32),
        pltpu.VMEM((second * BLOCK, first), F32),
        pltpu.SemaphoreType.DMA((3 + len(constants),)),
        pltpu.SemaphoreType.DMA((mixed // WIDE,)),
        pltpu.SemaphoreType.DMA((2,)),
        *[pltpu.SemaphoreType.DMA((tiles,)) for _ in range(4)],
    ]
    vmem = pl.BlockSpec(memory_space=pltpu.VMEM)
    made = pl.pallas_call(
        functools.partial(mixer_kernel, rows, cols),
        in_specs=[hbm] * len(operands),
        out_specs=[vmem] * 3,
        out_shape=[
            pltpu.VMEM(tokens.shape, BF16), pltpu.VMEM((tile, mixed), BF16), pltpu.VMEM(out_weight.shape, BF16)
        ],
        scratch_shapes=scratch,
        compiler_params=pltpu.CompilerParams(
            collective_id=0, has_side_effects=True, vmem_limit_bytes=48 * 2**20
        ),
        name="mixer",
    )(*operands)
    return pl.pallas_call(
        last_kernel,
        in_specs=[vmem] * 3,
        out_specs=hbm,
        out_shape=jax.ShapeDtypeStruct(tokens.shape, BF16),
        scratch_shapes=[pltpu.VMEM((tile, width), BF16), pltpu.SemaphoreType.DMA((tiles,))],
        compiler_params=pltpu.CompilerParams(vmem_limit_bytes=4 * 2**20),
        name="last",
    )(*[pltpu.with_memory_space_constraint(array, pltpu.VMEM) for array in made])


def fits(devices, tokens, mix_weight):
    seqs, here, width = tokens.shape
    mixed = mix_weight.shape[1]
    second = here * devices // GROUP_DIM
    return (
        devices % 16 == 0
        and GROUP_DIM % devices == 0
        and mixed % (devices * BLOCK) == 0
        and second % WIDE == 0
        and here % second == 0
        and here // second == GROUP_DIM // devices
        and mixed % WIDE == 0
        and width % WIDE == 0
    )


def local(rows, cols, tokens, norm_gain, mix_weight, gate_weight, out_weight):
    args = (tokens, norm_gain, mix_weight, gate_weight, out_weight)
    if fits(rows * cols, tokens, mix_weight):
        return fused(rows, cols, *args)
    return plain(rows * cols, *args)


def solution(mesh):
    in_specs = (P(None, AXES, None), P(), P(), P(), P())
    body = functools.partial(local, mesh.shape["row"], mesh.shape["col"])
    return jax.shard_map(body, mesh=mesh, in_specs=in_specs, out_specs=P(None, AXES, None), check_vma=False)
```

```python
import functools
import math

import jax
import jax.numpy as jnp
import numpy as np
from jax import lax
from jax.experimental import pallas as pl
from jax.experimental.pallas import tpu as pltpu
from jax.sharding import PartitionSpec as P

GROUP_DIM = 128
HALF = GROUP_DIM // 2
BF16 = jnp.bfloat16
F32 = jnp.float32
AXES = ("row", "col")
LANES = 128
BLOCK = 16
WIDE = 256
NT = (((1,), (1,)), ((), ()))
MESH = pl.DeviceIdType.MESH


def angles(left, right, period):
    return (np.outer(left, right) % period) * (2.0 * math.pi / period)


def channel_table():
    phase = angles(np.arange(GROUP_DIM), np.arange(HALF), GROUP_DIM)
    table = np.stack([np.cos(phase), np.sin(phase)], axis=-1)
    table[:, 0, 1] = np.cos(math.pi * np.arange(GROUP_DIM))
    return table.reshape(GROUP_DIM, GROUP_DIM) * GROUP_DIM ** -0.5


def channel_order():
    order = np.zeros((HALF, 2), np.int64)
    order[:, 0] = np.arange(HALF)
    order[:, 1] = GROUP_DIM - np.arange(HALF)
    order[0, 1] = HALF
    pick = np.zeros((GROUP_DIM, GROUP_DIM))
    pick[np.arange(GROUP_DIM), order.reshape(-1)] = 1.0
    return pick


def position_tables(devices, length, first):
    second, fold = length // first, first // devices
    phase = angles(np.arange(first), np.arange(first), first)
    cosine, sine = np.cos(phase), np.sin(phase)
    zero = np.zeros_like(cosine)
    from_left = np.concatenate([cosine, sine, cosine, sine], axis=1)
    from_right = np.concatenate([-sine, cosine, sine, -cosine], axis=1)
    lone_left = np.concatenate([cosine, sine, zero, zero], axis=1)
    lone_right = np.concatenate([zero, zero, cosine, sine], axis=1)

    def interleave(left, right):
        pair = np.stack([left, right]).reshape(2, devices, fold, -1).transpose(0, 2, 1, 3)
        return pair.reshape(2 * first, 4 * first)

    turn = angles(np.arange(second), np.arange(first), length)
    last = angles(np.arange(second), np.arange(second), second)
    closing = np.concatenate([np.cos(last), -np.sin(last)], axis=1) * length ** -0.5
    return (
        interleave(from_left, from_right),
        interleave(lone_left, lone_right),
        np.cos(turn),
        np.sin(turn),
        closing,
    )


def turn_halves(u, cosine, sine, first):
    halves = []
    for half in range(2):
        real = u[..., 2 * half * first : (2 * half + 1) * first]
        imag = u[..., (2 * half + 1) * first : (2 * half + 2) * first]
        halves.append(
            jnp.concatenate(
                [(real * cosine - imag * sine).astype(BF16), (real * sine + imag * cosine).astype(BF16)], axis=-2
            )
        )
    return jnp.concatenate(halves, axis=-1)


def position_transform(x, lone_here, devices, length, first):
    _, channels, here = x.shape
    second, fold = length // first, first // devices
    normal, lone, cosine, sine, closing = position_tables(devices, length, first)
    normal, lone = jnp.asarray(normal, BF16), jnp.asarray(lone, BF16)
    cosine, sine, closing = jnp.asarray(cosine, F32), jnp.asarray(sine, F32), jnp.asarray(closing, BF16)
    g = jnp.stack([jnp.where(lone_here, lone, normal), normal])
    pairs, span = channels // 2, min(first, here)
    x = x.reshape(devices, pairs, 2, fold, second).transpose(1, 2, 3, 0, 4).reshape(pairs, 2 * first, second)
    g = jnp.stack([g[min(pair, 1)] for pair in range(pairs)])
    u = jnp.einsum("pxr,pxj->prj", x, g, preferred_element_type=F32)
    y = jnp.einsum("kx,pxj->pkj", closing, turn_halves(u, cosine, sine, first), preferred_element_type=F32)
    y = y.astype(BF16).reshape(pairs, second, 2, first).transpose(1, 3, 0, 2)
    return y.reshape(devices, here // span, span, channels).transpose(0, 1, 3, 2)


def plain(devices, tokens, norm_gain, mix_weight, gate_weight, out_weight):
    seqs, here, width = tokens.shape
    length = here * devices
    mixed = mix_weight.shape[1]
    groups = mixed // GROUP_DIM
    channels = mixed // devices
    first = max(GROUP_DIM, devices)
    mix = jnp.einsum(
        "dgj,jk->dgk", mix_weight.reshape(width, groups, GROUP_DIM), jnp.asarray(channel_table(), BF16),
        preferred_element_type=F32,
    ).astype(BF16).reshape(width, mixed)
    ordered = jnp.einsum(
        "ij,gjd->gid", jnp.asarray(channel_order(), BF16), out_weight.reshape(groups, GROUP_DIM, width),
        preferred_element_type=F32,
    ).astype(BF16).reshape(mixed, width)
    widened = tokens.astype(F32)
    inverse_rms = lax.rsqrt(jnp.mean(widened * widened, axis=-1, keepdims=True) + 1e-06)
    normed = (widened * inverse_rms * norm_gain).astype(BF16)
    gate_value = jax.nn.sigmoid(jnp.dot(normed, gate_weight, preferred_element_type=F32)).astype(BF16)
    lone_here = lax.axis_index(AXES) * (channels // 2) % HALF == 0

    def exchange(x):
        return lax.all_to_all(x, AXES, split_axis=0, concat_axis=0, tiled=True)

    returned = []
    for seq in range(seqs):
        columns = lax.dot_general(
            mix, normed[seq], (((0,), (1,)), ((), ())), preferred_element_type=F32
        ).astype(BF16).reshape(devices, channels, here)
        returned.append(exchange(position_transform(exchange(columns), lone_here, devices, length, first)))
    spectral = jnp.stack(returned).transpose(0, 2, 4, 1, 3).reshape(seqs, here, mixed)
    mapped = jnp.dot(spectral, ordered, preferred_element_type=F32)
    return (gate_value * mapped).astype(BF16)


def mixer_kernel(
    rows, cols, tokens, gain_in, mix_in, gate_in, out_in, table_in, order_in, eye_in, spread_in, cos_in, sin_in,
    close_in, result, left_v, out_v, token_v, normed, mix_v, gate_v, gain_v, table_v, order_v, eye_v, spread_v, cos_v,
    sin_v, close_v, send_f, recv_f, send_r, recv_r, rows_in, rows_out, load_sem, mix_sem, token_sem, send_f_sem, recv_f_sem, send_r_sem, recv_r_sem, word,
):
    devices = rows * cols
    row, col = lax.axis_index("row"), lax.axis_index("col")
    me = row * cols + col
    tile, width = token_v.shape[1], token_v.shape[2]
    tiles = send_f.shape[0]
    seqs = tokens.shape[0]
    per_seq = tiles // seqs
    channels = send_f.shape[2]
    mixed = devices * channels
    first, second = cos_v.shape
    lows = send_r.shape[2]
    per_group = GROUP_DIM // channels

    barrier = pltpu.get_barrier_semaphore()

    span = WIDE // channels
    chunks = devices // span
    mine, within = me // span, lax.rem(me, span)

    def partner(chunk, k):
        there = chunk * span + lax.rem(within + k, span)
        return there, (there // cols, lax.rem(there, cols))

    last = chunks - 1
    relay = (last - 1) * span + 1
    relay_address = (relay // cols, relay % cols)

    def tell(chunk, semaphore):
        for k in range(span):
            there, address = partner(chunk, k)

            @pl.when(there != me)
            def _():
                pl.semaphore_signal(semaphore, inc=1, device_id=address, device_id_type=MESH)

    @pl.when(mine != last)
    def _():
        for shift in range(last):
            tell(lax.rem(2 * last - 1 - mine + shift, last), barrier)

    @pl.when(mine == last)
    def _():
        pl.semaphore_signal(barrier, inc=1, device_id=relay_address, device_id_type=MESH)

    def positions(i):
        return pl.ds(pl.multiple_of(lax.rem(i, per_seq) * tile, tile), tile)

    def token_load(i):
        slot = lax.rem(i, 2)
        return pltpu.make_async_copy(
            tokens.at[i // per_seq, positions(i), :], token_v.at[slot], token_sem.at[slot]
        )

    half = chunks // 2

    def shifted(step):
        return lax.rem(mine + jnp.where(step == 0, half, step + jnp.where(step >= half, 1, 0)), chunks)

    away = last - mine
    turn = jnp.where(away == half, 0, jnp.where(away == 0, last, jnp.where(away > half, away - 1, away)))

    def chunk_at(step):
        return jnp.where(step == last, last, shifted(step + jnp.where(step >= turn, 1, 0)))

    def chunk_back(step):
        passing = step + 1 + jnp.where(step + 1 >= half, 1, 0)
        return lax.rem(mine + jnp.where(step == last, 0, jnp.where(step == last - 1, half, passing)), chunks)

    def wide(n):
        return pl.ds(pl.multiple_of(n * WIDE, WIDE), WIDE)

    def mix_load(step):
        these = wide(chunk_at(step))
        return pltpu.make_async_copy(mix_in.at[:, these], mix_v.at[:, these], mix_sem.at[step])

    loads = [
        pltpu.make_async_copy(here, there, load_sem.at[at])
        for at, (here, there) in enumerate([
            (gain_in, gain_v), (table_in, table_v), (spread_in, spread_v), (cos_in, cos_v), (sin_in, sin_v),
            (close_in, close_v), (gate_in, gate_v), (out_in, out_v), (order_in, order_v), (eye_in, eye_v),
        ])
    ]
    token_load(0).start()
    loads[0].start()
    loads[1].start()
    for step in range(chunks):
        mix_load(step).start()
    token_load(1).start()

    def norm(i):
        slot = lax.rem(i, 2)
        token_load(i).wait()

        def strip(r, carry):
            at = pl.ds(pl.multiple_of(r * 32, 32), 32)
            widened = token_v[slot, at, :].astype(F32)
            inverse_rms = lax.rsqrt(jnp.mean(widened * widened, axis=-1, keepdims=True) + 1e-06)
            normed[i, at, :] = (widened * inverse_rms * gain_v[...]).astype(BF16)
            return carry

        lax.fori_loop(0, tile // 32, strip, 0)

    def send_chunk(send_ref, recv_ref, send_sem, recv_sem, i, chunk):
        def one(k, carry):
            there, address = partner(chunk, k)

            @pl.when(there != me)
            def _():
                pltpu.make_async_remote_copy(
                    src_ref=send_ref.at[i, there], dst_ref=recv_ref.at[i, me], send_sem=send_sem.at[i],
                    recv_sem=recv_sem.at[i], device_id=address, device_id_type=MESH,
                ).start()

            return carry

        lax.fori_loop(0, span, one, 0)

    def send(send_ref, recv_ref, send_sem, recv_sem, i):
        def one(step, carry):
            send_chunk(send_ref, recv_ref, send_sem, recv_sem, i, chunk_back(step))
            return carry

        recv_ref[i, me] = send_ref[i, me]
        lax.fori_loop(0, chunks, one, 0)

    def await_all(ref, sem, i):
        others = ref.at[i, pl.ds(0, devices - 1)]
        pltpu.make_async_copy(others, others, sem.at[i]).wait()

    def compute(m):
        i, step = m // chunks, lax.rem(m, chunks)

        @pl.when(step == 0)
        def _():
            norm(i)

            @pl.when(i + 2 < tiles)
            def _():
                token_load(i + 2).start()

        @pl.when(i == 0)
        def _():
            mix_load(step).wait()

        n = chunk_at(step)
        mixed_in = jnp.dot(normed[i], mix_v[:, wide(n)], preferred_element_type=F32).astype(BF16)
        for part in range(WIDE // GROUP_DIM):
            turned = lax.dot_general(
                table_v[...], mixed_in[:, part * GROUP_DIM : (part + 1) * GROUP_DIM], NT,
                preferred_element_type=F32,
            ).astype(BF16)
            send_f[i, pl.ds(n * span + part * per_group, per_group)] = turned.reshape(per_group, channels, tile)

    def post(m):
        i, n = m // chunks, chunk_at(lax.rem(m, chunks))

        @pl.when(n == mine)
        def _():
            recv_f[i, me] = send_f[i, me]

        @pl.when(jnp.logical_and(m == last, jnp.logical_and(mine != last, me != relay)))
        def _():
            pl.semaphore_wait(word, 1)

        send_chunk(send_f, recv_f, send_f_sem, recv_f_sem, i, n)

    def forward(m, carry):
        compute(m + 1)

        @pl.when(m > 0)
        def _():
            post(m)

        return carry

    pieces = tiles * chunks
    loads[0].wait()
    loads[1].wait()
    compute(0)
    for load in loads[2:]:
        load.start()

    @pl.when(me == relay)
    def _():
        pl.semaphore_wait(barrier, devices - 1)
        tell(last, barrier)
        for chunk in range(last):
            tell(chunk, word)

    @pl.when(jnp.logical_and(mine != last, me != relay))
    def _():
        pl.semaphore_wait(barrier, devices - span - 1)

    @pl.when(mine == last)
    def _():
        pl.semaphore_wait(barrier, 1)

    post(0)
    lax.fori_loop(0, pieces - 1, forward, 0)
    for load in loads[2:]:
        load.wait()
    post(pieces - 1)

    for group in range(mixed // GROUP_DIM):
        at = pl.ds(group * GROUP_DIM, GROUP_DIM)
        out_v[at, :] = jnp.dot(order_v[...], out_v[at, :], preferred_element_type=F32).astype(BF16)

    def transform(seq):
        def block(b, carry):
            these = pl.ds(pl.multiple_of(b * BLOCK, BLOCK), BLOCK)
            for t in range(per_seq):
                for half in range(tile // LANES):
                    rows_in[t * (tile // LANES) + half] = (
                        recv_f[seq * per_seq + t, :, these, half * LANES : (half + 1) * LANES]
                        .astype(F32).reshape(devices * BLOCK, LANES)
                    )
            for pair in range(BLOCK // 2):
                picked = []
                for column in range(2):
                    for t in range(per_seq):
                        at = pl.ds(2 * pair + column, devices, stride=BLOCK)
                        picked.append(
                            jnp.concatenate(
                                [rows_in[t * (tile // LANES) + half, at, :] for half in range(tile // LANES)], axis=1
                            ).astype(BF16)
                        )
                x = jnp.concatenate(picked, axis=0)
                if pair == 0:
                    lone = jnp.logical_and(b == 0, lax.rem(me, per_group) == 0)
                    spread = spread_v[jnp.where(lone, 0, 1)]
                else:
                    spread = spread_v[1]
                u = jnp.dot(spread, x, preferred_element_type=F32)
                cosine, sine = cos_v[...], sin_v[...]
                halves = []
                for half in range(2):
                    real = u[2 * half * first : (2 * half + 1) * first]
                    imag = u[(2 * half + 1) * first : (2 * half + 2) * first]
                    halves.append(
                        jnp.concatenate(
                            [(real * cosine - imag * sine).astype(BF16), (real * sine + imag * cosine).astype(BF16)],
                            axis=1,
                        )
                    )
                turned = jnp.concatenate(halves, axis=0)
                y = lax.dot_general(close_v[...], turned, NT, preferred_element_type=F32)
                for half in range(2):
                    rows_out[pl.ds(2 * pair + half, second, stride=BLOCK), :] = y[:, half * first : (half + 1) * first]

            def leave(there, carry):
                span = second // devices * BLOCK
                out = rows_out[pl.ds(pl.multiple_of(there * span, span), span), :].reshape(-1, BLOCK, LANES)
                for q in range(per_seq):
                    send_r[seq * per_seq + q, there, :, these, :] = out[q * lows : (q + 1) * lows].astype(BF16)
                return carry

            lax.fori_loop(0, devices, leave, 0)
            return carry

        lax.fori_loop(0, channels // BLOCK, block, 0)

    def middle(seq, carry):
        for t in range(per_seq):
            await_all(recv_f, recv_f_sem, seq * per_seq + t)
        transform(seq)
        def gate(at, carry):
            i, n = seq * per_seq + at // (width // WIDE), lax.rem(at, width // WIDE)
            these = wide(n)
            logits = jnp.dot(normed[i], gate_v[:, these], preferred_element_type=F32)
            result[seq, positions(i), these] = jax.nn.sigmoid(logits).astype(BF16)
            return carry

        lax.fori_loop(0, per_seq * (width // WIDE), gate, 0)
        for q in range(per_seq):
            send(send_r, recv_r, send_r_sem, recv_r_sem, seq * per_seq + q)
        return carry

    lax.fori_loop(0, seqs, middle, 0)

    def gather(j):
        await_all(recv_r, recv_r_sem, j)
        left = jnp.concatenate([recv_r[j, :, low].reshape(mixed, LANES) for low in range(lows)], axis=1)
        left_v[...] = lax.dot_general(eye_v[...], left, NT, preferred_element_type=F32).astype(BF16)

    def finish(j, carry):
        gather(j)

        def columns(n, carry):
            at = (j // per_seq, positions(j), wide(n))
            mapped = jnp.dot(left_v[...], out_v[:, wide(n)], preferred_element_type=F32)
            result[at] = (result[at].astype(F32) * mapped).astype(BF16)
            return carry

        lax.fori_loop(0, width // WIDE, columns, 0)
        return carry

    lax.fori_loop(0, tiles - 1, finish, 0)
    gather(tiles - 1)
    for i in range(tiles):
        await_all(send_f, send_f_sem, i)
        await_all(send_r, send_r_sem, i)


def last_kernel(gated, left, out_v, final, stage, sems):
    tile, width = stage.shape
    per_seq = gated.shape[1] // tile
    tiles = sems.shape[0]

    def put(j):
        at = (j // per_seq, pl.ds(j % per_seq * tile, tile))
        return pltpu.make_async_copy(gated.at[at] if j + 1 < tiles else stage, final.at[at], sems.at[j])

    for j in range(tiles - 1):
        put(j).start()

    def columns(n, carry):
        at = pl.ds(pl.multiple_of(n * WIDE, WIDE), WIDE)
        mapped = jnp.dot(left[...], out_v[:, at], preferred_element_type=F32)
        gate = gated[gated.shape[0] - 1, gated.shape[1] - tile :, at].astype(F32)
        stage[:, at] = (gate * mapped).astype(BF16)
        return carry

    lax.fori_loop(0, width // WIDE, columns, 0)
    put(tiles - 1).start()
    for j in range(tiles):
        put(j).wait()


def fused(rows, cols, tokens, norm_gain, mix_weight, gate_weight, out_weight):
    devices = rows * cols
    seqs, here, width = tokens.shape
    length = here * devices
    mixed = mix_weight.shape[1]
    channels = mixed // devices
    first = GROUP_DIM
    second = length // first
    tile = second
    tiles = seqs * here // tile
    lows = tile // first
    normal, lone, cosine, sine, closing = position_tables(devices, length, first)
    constants = [
        jnp.asarray(channel_table().T, BF16),
        jnp.asarray(channel_order(), BF16),
        jnp.asarray(np.eye(tile), BF16),
        jnp.asarray(np.stack([lone.T, normal.T]), BF16),
        jnp.asarray(cosine.T, F32),
        jnp.asarray(sine.T, F32),
        jnp.asarray(closing, BF16),
    ]
    operands = [tokens, norm_gain.reshape(1, width), mix_weight, gate_weight, out_weight, *constants]
    hbm = pl.BlockSpec(memory_space=pl.ANY)
    scratch = [
        pltpu.VMEM((2, tile, width), BF16),
        pltpu.VMEM((tiles, tile, width), BF16),
        pltpu.VMEM(mix_weight.shape, BF16),
        pltpu.VMEM(gate_weight.shape, BF16),
        pltpu.VMEM((1, width), F32),
        *[pltpu.VMEM(constant.shape, constant.dtype) for constant in constants],
        pltpu.VMEM((tiles, devices, channels, tile), BF16),
        pltpu.VMEM((tiles, devices, channels, tile), BF16),
        pltpu.VMEM((tiles, devices, lows, channels, first), BF16),
        pltpu.VMEM((tiles, devices, lows, channels, first), BF16),
        pltpu.VMEM((here // LANES, devices * BLOCK, LANES), F32),
        pltpu.VMEM((second * BLOCK, first), F32),
        pltpu.SemaphoreType.DMA((3 + len(constants),)),
        pltpu.SemaphoreType.DMA((mixed // WIDE,)),
        pltpu.SemaphoreType.DMA((2,)),
        *[pltpu.SemaphoreType.DMA((tiles,)) for _ in range(4)],
        pltpu.SemaphoreType.REGULAR,
    ]
    vmem = pl.BlockSpec(memory_space=pltpu.VMEM)
    made = pl.pallas_call(
        functools.partial(mixer_kernel, rows, cols),
        in_specs=[hbm] * len(operands),
        out_specs=[vmem] * 3,
        out_shape=[
            pltpu.VMEM(tokens.shape, BF16), pltpu.VMEM((tile, mixed), BF16), pltpu.VMEM(out_weight.shape, BF16)
        ],
        scratch_shapes=scratch,
        compiler_params=pltpu.CompilerParams(
            collective_id=0, has_side_effects=True, vmem_limit_bytes=48 * 2**20
        ),
        name="mixer",
    )(*operands)
    return pl.pallas_call(
        last_kernel,
        in_specs=[vmem] * 3,
        out_specs=hbm,
        out_shape=jax.ShapeDtypeStruct(tokens.shape, BF16),
        scratch_shapes=[pltpu.VMEM((tile, width), BF16), pltpu.SemaphoreType.DMA((tiles,))],
        compiler_params=pltpu.CompilerParams(vmem_limit_bytes=4 * 2**20),
        name="last",
    )(*[pltpu.with_memory_space_constraint(array, pltpu.VMEM) for array in made])


def fits(devices, tokens, mix_weight):
    seqs, here, width = tokens.shape
    mixed = mix_weight.shape[1]
    second = here * devices // GROUP_DIM
    return (
        devices % 16 == 0
        and GROUP_DIM % devices == 0
        and mixed % (devices * BLOCK) == 0
        and second % WIDE == 0
        and here % second == 0
        and here // second == GROUP_DIM // devices
        and mixed % WIDE == 0
        and mixed // WIDE >= 4
        and width % WIDE == 0
    )


def local(rows, cols, tokens, norm_gain, mix_weight, gate_weight, out_weight):
    args = (tokens, norm_gain, mix_weight, gate_weight, out_weight)
    if fits(rows * cols, tokens, mix_weight):
        return fused(rows, cols, *args)
    return plain(rows * cols, *args)


def solution(mesh):
    in_specs = (P(None, AXES, None), P(), P(), P(), P())
    body = functools.partial(local, mesh.shape["row"], mesh.shape["col"])
    return jax.shard_map(body, mesh=mesh, in_specs=in_specs, out_specs=P(None, AXES, None), check_vma=False)
```

```python
import functools
import math

import jax
import jax.numpy as jnp
import numpy as np
from jax import lax
from jax.experimental import pallas as pl
from jax.experimental.pallas import tpu as pltpu
from jax.sharding import PartitionSpec as P

GROUP_DIM = 128
HALF = GROUP_DIM // 2
BF16 = jnp.bfloat16
F32 = jnp.float32
AXES = ("row", "col")
LANES = 128
BLOCK = 16
WIDE = 256
NT = (((1,), (1,)), ((), ()))
MESH = pl.DeviceIdType.MESH


def angles(left, right, period):
    return (np.outer(left, right) % period) * (2.0 * math.pi / period)


def channel_table():
    phase = angles(np.arange(GROUP_DIM), np.arange(HALF), GROUP_DIM)
    table = np.stack([np.cos(phase), np.sin(phase)], axis=-1)
    table[:, 0, 1] = np.cos(math.pi * np.arange(GROUP_DIM))
    return table.reshape(GROUP_DIM, GROUP_DIM) * GROUP_DIM ** -0.5


def channel_order():
    order = np.zeros((HALF, 2), np.int64)
    order[:, 0] = np.arange(HALF)
    order[:, 1] = GROUP_DIM - np.arange(HALF)
    order[0, 1] = HALF
    pick = np.zeros((GROUP_DIM, GROUP_DIM))
    pick[np.arange(GROUP_DIM), order.reshape(-1)] = 1.0
    return pick


def position_tables(devices, length, first):
    second, fold = length // first, first // devices
    phase = angles(np.arange(first), np.arange(first), first)
    cosine, sine = np.cos(phase), np.sin(phase)
    zero = np.zeros_like(cosine)
    from_left = np.concatenate([cosine, sine, cosine, sine], axis=1)
    from_right = np.concatenate([-sine, cosine, sine, -cosine], axis=1)
    lone_left = np.concatenate([cosine, sine, zero, zero], axis=1)
    lone_right = np.concatenate([zero, zero, cosine, sine], axis=1)

    def interleave(left, right):
        pair = np.stack([left, right]).reshape(2, devices, fold, -1).transpose(0, 2, 1, 3)
        return pair.reshape(2 * first, 4 * first)

    turn = angles(np.arange(second), np.arange(first), length)
    last = angles(np.arange(second), np.arange(second), second)
    closing = np.concatenate([np.cos(last), -np.sin(last)], axis=1) * length ** -0.5
    return (
        interleave(from_left, from_right),
        interleave(lone_left, lone_right),
        np.cos(turn),
        np.sin(turn),
        closing,
    )


def turn_halves(u, cosine, sine, first):
    halves = []
    for half in range(2):
        real = u[..., 2 * half * first : (2 * half + 1) * first]
        imag = u[..., (2 * half + 1) * first : (2 * half + 2) * first]
        halves.append(
            jnp.concatenate(
                [(real * cosine - imag * sine).astype(BF16), (real * sine + imag * cosine).astype(BF16)], axis=-2
            )
        )
    return jnp.concatenate(halves, axis=-1)


def position_transform(x, lone_here, devices, length, first):
    _, channels, here = x.shape
    second, fold = length // first, first // devices
    normal, lone, cosine, sine, closing = position_tables(devices, length, first)
    normal, lone = jnp.asarray(normal, BF16), jnp.asarray(lone, BF16)
    cosine, sine, closing = jnp.asarray(cosine, F32), jnp.asarray(sine, F32), jnp.asarray(closing, BF16)
    g = jnp.stack([jnp.where(lone_here, lone, normal), normal])
    pairs, span = channels // 2, min(first, here)
    x = x.reshape(devices, pairs, 2, fold, second).transpose(1, 2, 3, 0, 4).reshape(pairs, 2 * first, second)
    g = jnp.stack([g[min(pair, 1)] for pair in range(pairs)])
    u = jnp.einsum("pxr,pxj->prj", x, g, preferred_element_type=F32)
    y = jnp.einsum("kx,pxj->pkj", closing, turn_halves(u, cosine, sine, first), preferred_element_type=F32)
    y = y.astype(BF16).reshape(pairs, second, 2, first).transpose(1, 3, 0, 2)
    return y.reshape(devices, here // span, span, channels).transpose(0, 1, 3, 2)


def plain(devices, tokens, norm_gain, mix_weight, gate_weight, out_weight):
    seqs, here, width = tokens.shape
    length = here * devices
    mixed = mix_weight.shape[1]
    groups = mixed // GROUP_DIM
    channels = mixed // devices
    first = max(GROUP_DIM, devices)
    mix = jnp.einsum(
        "dgj,jk->dgk", mix_weight.reshape(width, groups, GROUP_DIM), jnp.asarray(channel_table(), BF16),
        preferred_element_type=F32,
    ).astype(BF16).reshape(width, mixed)
    ordered = jnp.einsum(
        "ij,gjd->gid", jnp.asarray(channel_order(), BF16), out_weight.reshape(groups, GROUP_DIM, width),
        preferred_element_type=F32,
    ).astype(BF16).reshape(mixed, width)
    widened = tokens.astype(F32)
    inverse_rms = lax.rsqrt(jnp.mean(widened * widened, axis=-1, keepdims=True) + 1e-06)
    normed = (widened * inverse_rms * norm_gain).astype(BF16)
    gate_value = jax.nn.sigmoid(jnp.dot(normed, gate_weight, preferred_element_type=F32)).astype(BF16)
    lone_here = lax.axis_index(AXES) * (channels // 2) % HALF == 0

    def exchange(x):
        return lax.all_to_all(x, AXES, split_axis=0, concat_axis=0, tiled=True)

    returned = []
    for seq in range(seqs):
        columns = lax.dot_general(
            mix, normed[seq], (((0,), (1,)), ((), ())), preferred_element_type=F32
        ).astype(BF16).reshape(devices, channels, here)
        returned.append(exchange(position_transform(exchange(columns), lone_here, devices, length, first)))
    spectral = jnp.stack(returned).transpose(0, 2, 4, 1, 3).reshape(seqs, here, mixed)
    mapped = jnp.dot(spectral, ordered, preferred_element_type=F32)
    return (gate_value * mapped).astype(BF16)


def mixer_kernel(
    rows, cols, tokens, gain_in, mix_in, gate_in, out_in, table_in, order_in, eye_in, spread_in, cos_in, sin_in,
    close_in, result, left_v, out_v, token_v, normed, mix_v, gate_v, gain_v, table_v, order_v, eye_v, spread_v, cos_v,
    sin_v, close_v, send_f, recv_f, send_r, recv_r, rows_in, rows_out, load_sem, mix_sem, token_sem, send_f_sem, recv_f_sem, send_r_sem, recv_r_sem, word,
):
    devices = rows * cols
    row, col = lax.axis_index("row"), lax.axis_index("col")
    me = row * cols + col
    tile, width = token_v.shape[1], token_v.shape[2]
    tiles = send_f.shape[0]
    seqs = tokens.shape[0]
    per_seq = tiles // seqs
    channels = send_f.shape[2]
    mixed = devices * channels
    first, second = cos_v.shape
    lows = send_r.shape[2]
    per_group = GROUP_DIM // channels

    barrier = pltpu.get_barrier_semaphore()

    span = WIDE // channels
    chunks = devices // span
    mine, within = me // span, lax.rem(me, span)

    def partner(chunk, k):
        there = chunk * span + lax.rem(within + k, span)
        return there, (there // cols, lax.rem(there, cols))

    last = chunks - 1
    relay = (last - 1) * span + 1
    relay_address = (relay // cols, relay % cols)

    def tell(chunk, semaphore):
        for k in range(span):
            there, address = partner(chunk, k)

            @pl.when(there != me)
            def _():
                pl.semaphore_signal(semaphore, inc=1, device_id=address, device_id_type=MESH)

    def positions(i):
        return pl.ds(pl.multiple_of(lax.rem(i, per_seq) * tile, tile), tile)

    def token_load(i):
        slot = lax.rem(i, 2)
        return pltpu.make_async_copy(
            tokens.at[i // per_seq, positions(i), :], token_v.at[slot], token_sem.at[slot]
        )

    half = chunks // 2

    def shifted(step):
        return lax.rem(mine + jnp.where(step == 0, half, step + jnp.where(step >= half, 1, 0)), chunks)

    away = last - mine
    turn = jnp.where(away == half, 0, jnp.where(away == 0, last, jnp.where(away > half, away - 1, away)))

    def chunk_first(step):
        return jnp.where(step == last, last, shifted(step + jnp.where(step >= turn, 1, 0)))

    def chunk_at(i, step):
        return jnp.where(i == 0, chunk_first(step), shifted(step))

    def chunk_back(step):
        passing = step + 1 + jnp.where(step + 1 >= half, 1, 0)
        return shifted(step)

    def wide(n):
        return pl.ds(pl.multiple_of(n * WIDE, WIDE), WIDE)

    def mix_load(step):
        these = wide(chunk_first(step))
        return pltpu.make_async_copy(mix_in.at[:, these], mix_v.at[:, these], mix_sem.at[step])

    loads = [
        pltpu.make_async_copy(here, there, load_sem.at[at])
        for at, (here, there) in enumerate([
            (gain_in, gain_v), (table_in, table_v), (spread_in, spread_v), (cos_in, cos_v), (sin_in, sin_v),
            (close_in, close_v), (gate_in, gate_v), (out_in, out_v), (order_in, order_v), (eye_in, eye_v),
        ])
    ]
    token_load(0).start()
    loads[0].start()
    loads[1].start()
    mix_load(0).start()

    @pl.when(mine != last)
    def _():
        for shift in range(last):
            tell(lax.rem(2 * last - 1 - mine + shift, last), barrier)

    @pl.when(mine == last)
    def _():
        pl.semaphore_signal(barrier, inc=1, device_id=relay_address, device_id_type=MESH)

    for step in range(1, chunks):
        mix_load(step).start()
    token_load(1).start()

    def norm(i):
        slot = lax.rem(i, 2)
        token_load(i).wait()

        def strip(r, carry):
            at = pl.ds(pl.multiple_of(r * 32, 32), 32)
            widened = token_v[slot, at, :].astype(F32)
            inverse_rms = lax.rsqrt(jnp.mean(widened * widened, axis=-1, keepdims=True) + 1e-06)
            normed[i, at, :] = (widened * inverse_rms * gain_v[...]).astype(BF16)
            return carry

        lax.fori_loop(0, tile // 32, strip, 0, unroll=4)

    def send_chunk(send_ref, recv_ref, send_sem, recv_sem, i, chunk):
        def one(k, carry):
            there, address = partner(chunk, k)

            @pl.when(there != me)
            def _():
                pltpu.make_async_remote_copy(
                    src_ref=send_ref.at[i, there], dst_ref=recv_ref.at[i, me], send_sem=send_sem.at[i],
                    recv_sem=recv_sem.at[i], device_id=address, device_id_type=MESH,
                ).start()

            return carry

        lax.fori_loop(0, span, one, 0)

    def send(send_ref, recv_ref, send_sem, recv_sem, i):
        def one(step, carry):
            send_chunk(send_ref, recv_ref, send_sem, recv_sem, i, chunk_back(step))
            return carry

        recv_ref[i, me] = send_ref[i, me]
        lax.fori_loop(0, chunks, one, 0)

    def await_all(ref, sem, i):
        others = ref.at[i, pl.ds(0, devices - 1)]
        pltpu.make_async_copy(others, others, sem.at[i]).wait()

    def compute(m):
        i, step = m // chunks, lax.rem(m, chunks)

        @pl.when(step == 0)
        def _():
            norm(i)

            @pl.when(i + 2 < tiles)
            def _():
                token_load(i + 2).start()

        @pl.when(i == 0)
        def _():
            mix_load(step).wait()

        n = chunk_at(i, step)
        mixed_in = jnp.dot(normed[i], mix_v[:, wide(n)], preferred_element_type=F32).astype(BF16)
        for part in range(WIDE // GROUP_DIM):
            turned = lax.dot_general(
                table_v[...], mixed_in[:, part * GROUP_DIM : (part + 1) * GROUP_DIM], NT,
                preferred_element_type=F32,
            ).astype(BF16)
            send_f[i, pl.ds(n * span + part * per_group, per_group)] = turned.reshape(per_group, channels, tile)

    def post(m):
        i, n = m // chunks, chunk_at(m // chunks, lax.rem(m, chunks))

        @pl.when(n == mine)
        def _():
            recv_f[i, me] = send_f[i, me]

        @pl.when(jnp.logical_and(m == last, jnp.logical_and(mine != last, me != relay)))
        def _():
            pl.semaphore_wait(word, 1)

        send_chunk(send_f, recv_f, send_f_sem, recv_f_sem, i, n)

    def forward(m, carry):
        compute(m + 1)

        @pl.when(m > 0)
        def _():
            post(m)

        return carry

    pieces = tiles * chunks
    loads[0].wait()
    loads[1].wait()
    compute(0)
    for load in loads[2:]:
        load.start()

    @pl.when(me == relay)
    def _():
        pl.semaphore_wait(barrier, devices - 1)
        tell(last, barrier)
        for chunk in range(last):
            tell(chunk, word)

    @pl.when(jnp.logical_and(mine != last, me != relay))
    def _():
        pl.semaphore_wait(barrier, devices - span - 1)

    @pl.when(mine == last)
    def _():
        pl.semaphore_wait(barrier, 1)

    post(0)
    lax.fori_loop(0, pieces - 1, forward, 0)
    for load in loads[2:]:
        load.wait()
    post(pieces - 1)

    for group in range(mixed // GROUP_DIM):
        at = pl.ds(group * GROUP_DIM, GROUP_DIM)
        out_v[at, :] = jnp.dot(order_v[...], out_v[at, :], preferred_element_type=F32).astype(BF16)

    def transform(seq):
        def block(b, carry):
            these = pl.ds(pl.multiple_of(b * BLOCK, BLOCK), BLOCK)
            for t in range(per_seq):
                for half in range(tile // LANES):
                    rows_in[t * (tile // LANES) + half] = (
                        recv_f[seq * per_seq + t, :, these, half * LANES : (half + 1) * LANES]
                        .astype(F32).reshape(devices * BLOCK, LANES)
                    )
            for pair in range(BLOCK // 2):
                picked = []
                for column in range(2):
                    for t in range(per_seq):
                        at = pl.ds(2 * pair + column, devices, stride=BLOCK)
                        picked.append(
                            jnp.concatenate(
                                [rows_in[t * (tile // LANES) + half, at, :] for half in range(tile // LANES)], axis=1
                            ).astype(BF16)
                        )
                x = jnp.concatenate(picked, axis=0)
                if pair == 0:
                    lone = jnp.logical_and(b == 0, lax.rem(me, per_group) == 0)
                    spread = spread_v[jnp.where(lone, 0, 1)]
                else:
                    spread = spread_v[1]
                u = jnp.dot(spread, x, preferred_element_type=F32)
                cosine, sine = cos_v[...], sin_v[...]
                halves = []
                for half in range(2):
                    real = u[2 * half * first : (2 * half + 1) * first]
                    imag = u[(2 * half + 1) * first : (2 * half + 2) * first]
                    halves.append(
                        jnp.concatenate(
                            [(real * cosine - imag * sine).astype(BF16), (real * sine + imag * cosine).astype(BF16)],
                            axis=1,
                        )
                    )
                turned = jnp.concatenate(halves, axis=0)
                y = lax.dot_general(close_v[...], turned, NT, preferred_element_type=F32)
                for half in range(2):
                    rows_out[pl.ds(2 * pair + half, second, stride=BLOCK), :] = y[:, half * first : (half + 1) * first]

            def leave(there, carry):
                span = second // devices * BLOCK
                out = rows_out[pl.ds(pl.multiple_of(there * span, span), span), :].reshape(-1, BLOCK, LANES)
                for q in range(per_seq):
                    send_r[seq * per_seq + q, there, :, these, :] = out[q * lows : (q + 1) * lows].astype(BF16)
                return carry

            lax.fori_loop(0, devices, leave, 0)
            return carry

        lax.fori_loop(0, channels // BLOCK, block, 0)

    def middle(seq, carry):
        for t in range(per_seq):
            await_all(recv_f, recv_f_sem, seq * per_seq + t)
        transform(seq)
        def gate(at, carry):
            i, n = seq * per_seq + at // (width // WIDE), lax.rem(at, width // WIDE)
            these = wide(n)
            logits = jnp.dot(normed[i], gate_v[:, these], preferred_element_type=F32)
            result[seq, positions(i), these] = jax.nn.sigmoid(logits).astype(BF16)
            return carry

        lax.fori_loop(0, per_seq * (width // WIDE), gate, 0)
        for q in range(per_seq):
            send(send_r, recv_r, send_r_sem, recv_r_sem, seq * per_seq + q)
        return carry

    lax.fori_loop(0, seqs, middle, 0)

    def gather(j):
        await_all(recv_r, recv_r_sem, j)
        left = jnp.concatenate([recv_r[j, :, low].reshape(mixed, LANES) for low in range(lows)], axis=1)
        left_v[...] = lax.dot_general(eye_v[...], left, NT, preferred_element_type=F32).astype(BF16)

    def finish(j, carry):
        gather(j)

        def columns(n, carry):
            at = (j // per_seq, positions(j), wide(n))
            mapped = jnp.dot(left_v[...], out_v[:, wide(n)], preferred_element_type=F32)
            result[at] = (result[at].astype(F32) * mapped).astype(BF16)
            return carry

        lax.fori_loop(0, width // WIDE, columns, 0)
        return carry

    lax.fori_loop(0, tiles - 1, finish, 0)
    gather(tiles - 1)
    for i in range(tiles):
        await_all(send_f, send_f_sem, i)
        await_all(send_r, send_r_sem, i)


def last_kernel(gated, left, out_v, final, stage, sems):
    tile, width = stage.shape
    per_seq = gated.shape[1] // tile
    tiles = sems.shape[0]

    def put(j):
        at = (j // per_seq, pl.ds(j % per_seq * tile, tile))
        return pltpu.make_async_copy(gated.at[at] if j + 1 < tiles else stage, final.at[at], sems.at[j])

    for j in range(tiles - 1):
        put(j).start()

    def columns(n, carry):
        at = pl.ds(pl.multiple_of(n * WIDE, WIDE), WIDE)
        mapped = jnp.dot(left[...], out_v[:, at], preferred_element_type=F32)
        gate = gated[gated.shape[0] - 1, gated.shape[1] - tile :, at].astype(F32)
        stage[:, at] = (gate * mapped).astype(BF16)
        return carry

    lax.fori_loop(0, width // WIDE, columns, 0)
    put(tiles - 1).start()
    for j in range(tiles):
        put(j).wait()


def fused(rows, cols, tokens, norm_gain, mix_weight, gate_weight, out_weight):
    devices = rows * cols
    seqs, here, width = tokens.shape
    length = here * devices
    mixed = mix_weight.shape[1]
    channels = mixed // devices
    first = GROUP_DIM
    second = length // first
    tile = second
    tiles = seqs * here // tile
    lows = tile // first
    normal, lone, cosine, sine, closing = position_tables(devices, length, first)
    constants = [
        jnp.asarray(channel_table().T, BF16),
        jnp.asarray(channel_order(), BF16),
        jnp.asarray(np.eye(tile), BF16),
        jnp.asarray(np.stack([lone.T, normal.T]), BF16),
        jnp.asarray(cosine.T, F32),
        jnp.asarray(sine.T, F32),
        jnp.asarray(closing, BF16),
    ]
    operands = [tokens, norm_gain.reshape(1, width), mix_weight, gate_weight, out_weight, *constants]
    hbm = pl.BlockSpec(memory_space=pl.ANY)
    scratch = [
        pltpu.VMEM((2, tile, width), BF16),
        pltpu.VMEM((tiles, tile, width), BF16),
        pltpu.VMEM(mix_weight.shape, BF16),
        pltpu.VMEM(gate_weight.shape, BF16),
        pltpu.VMEM((1, width), F32),
        *[pltpu.VMEM(constant.shape, constant.dtype) for constant in constants],
        pltpu.VMEM((tiles, devices, channels, tile), BF16),
        pltpu.VMEM((tiles, devices, channels, tile), BF16),
        pltpu.VMEM((tiles, devices, lows, channels, first), BF16),
        pltpu.VMEM((tiles, devices, lows, channels, first), BF16),
        pltpu.VMEM((here // LANES, devices * BLOCK, LANES), F32),
        pltpu.VMEM((second * BLOCK, first), F32),
        pltpu.SemaphoreType.DMA((3 + len(constants),)),
        pltpu.SemaphoreType.DMA((mixed // WIDE,)),
        pltpu.SemaphoreType.DMA((2,)),
        *[pltpu.SemaphoreType.DMA((tiles,)) for _ in range(4)],
        pltpu.SemaphoreType.REGULAR,
    ]
    vmem = pl.BlockSpec(memory_space=pltpu.VMEM)
    made = pl.pallas_call(
        functools.partial(mixer_kernel, rows, cols),
        in_specs=[hbm] * len(operands),
        out_specs=[vmem] * 3,
        out_shape=[
            pltpu.VMEM(tokens.shape, BF16), pltpu.VMEM((tile, mixed), BF16), pltpu.VMEM(out_weight.shape, BF16)
        ],
        scratch_shapes=scratch,
        compiler_params=pltpu.CompilerParams(
            collective_id=0, has_side_effects=True, vmem_limit_bytes=48 * 2**20
        ),
        name="mixer",
    )(*operands)
    return pl.pallas_call(
        last_kernel,
        in_specs=[vmem] * 3,
        out_specs=hbm,
        out_shape=jax.ShapeDtypeStruct(tokens.shape, BF16),
        scratch_shapes=[pltpu.VMEM((tile, width), BF16), pltpu.SemaphoreType.DMA((tiles,))],
        compiler_params=pltpu.CompilerParams(vmem_limit_bytes=4 * 2**20),
        name="last",
    )(*[pltpu.with_memory_space_constraint(array, pltpu.VMEM) for array in made])


def fits(devices, tokens, mix_weight):
    seqs, here, width = tokens.shape
    mixed = mix_weight.shape[1]
    second = here * devices // GROUP_DIM
    return (
        devices % 16 == 0
        and GROUP_DIM % devices == 0
        and mixed % (devices * BLOCK) == 0
        and second % WIDE == 0
        and here % second == 0
        and here // second == GROUP_DIM // devices
        and mixed % WIDE == 0
        and mixed // WIDE >= 4
        and width % WIDE == 0
    )


def local(rows, cols, tokens, norm_gain, mix_weight, gate_weight, out_weight):
    args = (tokens, norm_gain, mix_weight, gate_weight, out_weight)
    if fits(rows * cols, tokens, mix_weight):
        return fused(rows, cols, *args)
    return plain(rows * cols, *args)


def solution(mesh):
    in_specs = (P(None, AXES, None), P(), P(), P(), P())
    body = functools.partial(local, mesh.shape["row"], mesh.shape["col"])
    return jax.shard_map(body, mesh=mesh, in_specs=in_specs, out_specs=P(None, AXES, None), check_vma=False)
```

```python
import functools
import math

import jax
import jax.numpy as jnp
import numpy as np
from jax import lax
from jax.experimental import pallas as pl
from jax.experimental.pallas import tpu as pltpu
from jax.sharding import PartitionSpec as P

GROUP_DIM = 128
HALF = GROUP_DIM // 2
BF16 = jnp.bfloat16
F32 = jnp.float32
AXES = ("row", "col")
LANES = 128
BLOCK = 16
WIDE = 256
NT = (((1,), (1,)), ((), ()))
MESH = pl.DeviceIdType.MESH


def angles(left, right, period):
    return (np.outer(left, right) % period) * (2.0 * math.pi / period)


def channel_table():
    phase = angles(np.arange(GROUP_DIM), np.arange(HALF), GROUP_DIM)
    table = np.stack([np.cos(phase), np.sin(phase)], axis=-1)
    table[:, 0, 1] = np.cos(math.pi * np.arange(GROUP_DIM))
    return table.reshape(GROUP_DIM, GROUP_DIM) * GROUP_DIM ** -0.5


def channel_order():
    order = np.zeros((HALF, 2), np.int64)
    order[:, 0] = np.arange(HALF)
    order[:, 1] = GROUP_DIM - np.arange(HALF)
    order[0, 1] = HALF
    pick = np.zeros((GROUP_DIM, GROUP_DIM))
    pick[np.arange(GROUP_DIM), order.reshape(-1)] = 1.0
    return pick


def position_tables(devices, length, first):
    second, fold = length // first, first // devices
    phase = angles(np.arange(first), np.arange(first), first)
    cosine, sine = np.cos(phase), np.sin(phase)
    zero = np.zeros_like(cosine)
    from_left = np.concatenate([cosine, sine, cosine, sine], axis=1)
    from_right = np.concatenate([-sine, cosine, sine, -cosine], axis=1)
    lone_left = np.concatenate([cosine, sine, zero, zero], axis=1)
    lone_right = np.concatenate([zero, zero, cosine, sine], axis=1)

    def interleave(left, right):
        pair = np.stack([left, right]).reshape(2, devices, fold, -1).transpose(0, 2, 1, 3)
        return pair.reshape(2 * first, 4 * first)

    turn = angles(np.arange(second), np.arange(first), length)
    last = angles(np.arange(second), np.arange(second), second)
    closing = np.concatenate([np.cos(last), -np.sin(last)], axis=1) * length ** -0.5
    return (
        interleave(from_left, from_right),
        interleave(lone_left, lone_right),
        np.cos(turn),
        np.sin(turn),
        closing,
    )


def turn_halves(u, cosine, sine, first):
    halves = []
    for half in range(2):
        real = u[..., 2 * half * first : (2 * half + 1) * first]
        imag = u[..., (2 * half + 1) * first : (2 * half + 2) * first]
        halves.append(
            jnp.concatenate(
                [(real * cosine - imag * sine).astype(BF16), (real * sine + imag * cosine).astype(BF16)], axis=-2
            )
        )
    return jnp.concatenate(halves, axis=-1)


def position_transform(x, lone_here, devices, length, first):
    _, channels, here = x.shape
    second, fold = length // first, first // devices
    normal, lone, cosine, sine, closing = position_tables(devices, length, first)
    normal, lone = jnp.asarray(normal, BF16), jnp.asarray(lone, BF16)
    cosine, sine, closing = jnp.asarray(cosine, F32), jnp.asarray(sine, F32), jnp.asarray(closing, BF16)
    g = jnp.stack([jnp.where(lone_here, lone, normal), normal])
    pairs, span = channels // 2, min(first, here)
    x = x.reshape(devices, pairs, 2, fold, second).transpose(1, 2, 3, 0, 4).reshape(pairs, 2 * first, second)
    g = jnp.stack([g[min(pair, 1)] for pair in range(pairs)])
    u = jnp.einsum("pxr,pxj->prj", x, g, preferred_element_type=F32)
    y = jnp.einsum("kx,pxj->pkj", closing, turn_halves(u, cosine, sine, first), preferred_element_type=F32)
    y = y.astype(BF16).reshape(pairs, second, 2, first).transpose(1, 3, 0, 2)
    return y.reshape(devices, here // span, span, channels).transpose(0, 1, 3, 2)


def plain(devices, tokens, norm_gain, mix_weight, gate_weight, out_weight):
    seqs, here, width = tokens.shape
    length = here * devices
    mixed = mix_weight.shape[1]
    groups = mixed // GROUP_DIM
    channels = mixed // devices
    first = max(GROUP_DIM, devices)
    mix = jnp.einsum(
        "dgj,jk->dgk", mix_weight.reshape(width, groups, GROUP_DIM), jnp.asarray(channel_table(), BF16),
        preferred_element_type=F32,
    ).astype(BF16).reshape(width, mixed)
    ordered = jnp.einsum(
        "ij,gjd->gid", jnp.asarray(channel_order(), BF16), out_weight.reshape(groups, GROUP_DIM, width),
        preferred_element_type=F32,
    ).astype(BF16).reshape(mixed, width)
    widened = tokens.astype(F32)
    inverse_rms = lax.rsqrt(jnp.mean(widened * widened, axis=-1, keepdims=True) + 1e-06)
    normed = (widened * inverse_rms * norm_gain).astype(BF16)
    gate_value = jax.nn.sigmoid(jnp.dot(normed, gate_weight, preferred_element_type=F32)).astype(BF16)
    lone_here = lax.axis_index(AXES) * (channels // 2) % HALF == 0

    def exchange(x):
        return lax.all_to_all(x, AXES, split_axis=0, concat_axis=0, tiled=True)

    returned = []
    for seq in range(seqs):
        columns = lax.dot_general(
            mix, normed[seq], (((0,), (1,)), ((), ())), preferred_element_type=F32
        ).astype(BF16).reshape(devices, channels, here)
        returned.append(exchange(position_transform(exchange(columns), lone_here, devices, length, first)))
    spectral = jnp.stack(returned).transpose(0, 2, 4, 1, 3).reshape(seqs, here, mixed)
    mapped = jnp.dot(spectral, ordered, preferred_element_type=F32)
    return (gate_value * mapped).astype(BF16)


def mixer_kernel(
    rows, cols, tokens, gain_in, mix_in, gate_in, out_in, table_in, order_in, eye_in, spread_in, cos_in, sin_in,
    close_in, result, left_v, out_v, token_v, normed, mix_v, gate_v, gain_v, table_v, order_v, eye_v, spread_v, cos_v,
    sin_v, close_v, send_f, recv_f, send_r, recv_r, rows_in, rows_out, load_sem, mix_sem, token_sem, send_f_sem, recv_f_sem, send_r_sem, recv_r_sem, word,
):
    devices = rows * cols
    row, col = lax.axis_index("row"), lax.axis_index("col")
    me = row * cols + col
    tile, width = token_v.shape[1], token_v.shape[2]
    tiles = send_f.shape[0]
    seqs = tokens.shape[0]
    per_seq = tiles // seqs
    channels = send_f.shape[2]
    mixed = devices * channels
    first, second = cos_v.shape
    lows = send_r.shape[2]
    per_group = GROUP_DIM // channels

    barrier = pltpu.get_barrier_semaphore()

    span = WIDE // channels
    chunks = devices // span
    mine, within = me // span, lax.rem(me, span)

    def partner(chunk, k):
        there = chunk * span + lax.rem(within + k, span)
        return there, (there // cols, lax.rem(there, cols))

    last = chunks - 1
    relay = last * span - 1
    relay_address = (relay // cols, relay % cols)

    def tell(chunk, semaphore):
        for k in range(span):
            there, address = partner(chunk, k)

            @pl.when(there != me)
            def _():
                pl.semaphore_signal(semaphore, inc=1, device_id=address, device_id_type=MESH)

    def positions(i):
        return pl.ds(pl.multiple_of(lax.rem(i, per_seq) * tile, tile), tile)

    def token_load(i):
        slot = lax.rem(i, 2)
        return pltpu.make_async_copy(
            tokens.at[i // per_seq, positions(i), :], token_v.at[slot], token_sem.at[slot]
        )

    half = chunks // 2

    def shifted(step):
        return lax.rem(mine + jnp.where(step == 0, half, step + jnp.where(step >= half, 1, 0)), chunks)

    away = last - mine
    turn = jnp.where(away == half, 0, jnp.where(away == 0, last, jnp.where(away > half, away - 1, away)))

    def chunk_first(step):
        return jnp.where(step == last, last, shifted(step + jnp.where(step >= turn, 1, 0)))

    def chunk_at(i, step):
        return jnp.where(i == 0, chunk_first(step), shifted(step))

    def chunk_back(step):
        passing = step + 1 + jnp.where(step + 1 >= half, 1, 0)
        return shifted(step)

    def wide(n):
        return pl.ds(pl.multiple_of(n * WIDE, WIDE), WIDE)

    fore = tile // 2

    def token_half(part):
        rows_at = pl.ds(part * fore, fore)
        return pltpu.make_async_copy(tokens.at[0, rows_at, :], token_v.at[0, rows_at, :], token_sem.at[2 * part])

    def mix_load(step):
        these = wide(chunk_first(step))
        return pltpu.make_async_copy(mix_in.at[:, these], mix_v.at[:, these], mix_sem.at[step])

    loads = [
        pltpu.make_async_copy(here, there, load_sem.at[at])
        for at, (here, there) in enumerate([
            (gain_in, gain_v), (table_in, table_v), (spread_in, spread_v), (cos_in, cos_v), (sin_in, sin_v),
            (close_in, close_v), (gate_in, gate_v), (out_in, out_v), (order_in, order_v), (eye_in, eye_v),
        ])
    ]
    token_half(0).start()
    loads[0].start()
    loads[1].start()
    mix_load(0).start()
    token_half(1).start()

    @pl.when(mine != last)
    def _():
        for shift in range(last):
            tell(lax.rem(2 * last - 1 - mine + shift, last), barrier)

    @pl.when(mine == last)
    def _():
        pl.semaphore_signal(barrier, inc=1, device_id=relay_address, device_id_type=MESH)

    for step in range(1, chunks):
        mix_load(step).start()
    token_load(1).start()

    def strip_of(i, r):
        slot = lax.rem(i, 2)
        at = pl.ds(pl.multiple_of(r * 32, 32), 32)
        widened = token_v[slot, at, :].astype(F32)
        inverse_rms = lax.rsqrt(jnp.mean(widened * widened, axis=-1, keepdims=True) + 1e-06)
        normed[i, at, :] = (widened * inverse_rms * gain_v[...]).astype(BF16)

    def norm(i, low, high):
        def strip(r, carry):
            strip_of(i, r)
            return carry

        lax.fori_loop(low // 32, high // 32, strip, 0, unroll=4)

    def norm_tile(i):
        token_load(i).wait()
        norm(i, 0, tile)

    def send_chunk(send_ref, recv_ref, send_sem, recv_sem, i, chunk):
        def one(k, carry):
            there, address = partner(chunk, k)

            @pl.when(there != me)
            def _():
                pltpu.make_async_remote_copy(
                    src_ref=send_ref.at[i, there], dst_ref=recv_ref.at[i, me], send_sem=send_sem.at[i],
                    recv_sem=recv_sem.at[i], device_id=address, device_id_type=MESH,
                ).start()

            return carry

        lax.fori_loop(0, span, one, 0)

    def send(send_ref, recv_ref, send_sem, recv_sem, i):
        def one(step, carry):
            send_chunk(send_ref, recv_ref, send_sem, recv_sem, i, chunk_back(step))
            return carry

        recv_ref[i, me] = send_ref[i, me]
        lax.fori_loop(0, chunks, one, 0)

    def await_all(ref, sem, i):
        others = ref.at[i, pl.ds(0, devices - 1)]
        pltpu.make_async_copy(others, others, sem.at[i]).wait()

    def project(i, n, low, high):
        mixed_in = jnp.dot(normed[i, low:high, :], mix_v[:, wide(n)], preferred_element_type=F32).astype(BF16)
        for part in range(WIDE // GROUP_DIM):
            turned = lax.dot_general(
                table_v[...], mixed_in[:, part * GROUP_DIM : (part + 1) * GROUP_DIM], NT,
                preferred_element_type=F32,
            ).astype(BF16)
            owners = pl.ds(n * span + part * per_group, per_group)
            send_f[i, owners, :, low:high] = turned.reshape(per_group, channels, high - low)

    def compute(m):
        i, step = m // chunks, lax.rem(m, chunks)

        @pl.when(step == 0)
        def _():
            norm_tile(i)

            @pl.when(i + 2 < tiles)
            def _():
                token_load(i + 2).start()

        @pl.when(i == 0)
        def _():
            mix_load(step).wait()

        project(i, chunk_at(i, step), 0, tile)

    def compute_half(part):
        token_half(part).wait()
        norm(0, part * fore, (part + 1) * fore)
        if part == 0:
            mix_load(0).wait()
        project(0, chunk_first(0), part * fore, (part + 1) * fore)

    def post_half(part):
        lanes = pl.ds(part * fore, fore)

        def one(k, carry):
            there, address = partner(chunk_first(0), k)

            @pl.when(there != me)
            def _():
                pltpu.make_async_remote_copy(
                    src_ref=send_f.at[0, there, :, lanes], dst_ref=recv_f.at[0, me, :, lanes],
                    send_sem=send_f_sem.at[0], recv_sem=recv_f_sem.at[0], device_id=address, device_id_type=MESH,
                ).start()

            return carry

        lax.fori_loop(0, span, one, 0)

    def post(m):
        i, n = m // chunks, chunk_at(m // chunks, lax.rem(m, chunks))

        @pl.when(n == mine)
        def _():
            recv_f[i, me] = send_f[i, me]

        @pl.when(jnp.logical_and(m == last, jnp.logical_and(mine != last, me != relay)))
        def _():
            pl.semaphore_wait(word, 1)

        send_chunk(send_f, recv_f, send_f_sem, recv_f_sem, i, n)

    def forward(m, carry):
        compute(m + 1)

        @pl.when(m == 0)
        def _():
            post_half(1)

        @pl.when(m > 0)
        def _():
            post(m)

        return carry

    pieces = tiles * chunks
    loads[0].wait()
    loads[1].wait()
    compute_half(0)
    for load in loads[2:]:
        load.start()

    @pl.when(me == relay)
    def _():
        pl.semaphore_wait(barrier, devices - 1)
        tell(last, barrier)
        for chunk in range(last):
            tell(chunk, word)

    @pl.when(jnp.logical_and(mine != last, me != relay))
    def _():
        pl.semaphore_wait(barrier, devices - span - 1)

    @pl.when(mine == last)
    def _():
        pl.semaphore_wait(barrier, 1)

    post_half(0)
    compute_half(1)
    token_load(2).start()
    lax.fori_loop(0, pieces - 1, forward, 0)
    for load in loads[2:]:
        load.wait()
    post(pieces - 1)

    for group in range(mixed // GROUP_DIM):
        at = pl.ds(group * GROUP_DIM, GROUP_DIM)
        out_v[at, :] = jnp.dot(order_v[...], out_v[at, :], preferred_element_type=F32).astype(BF16)

    def transform(seq):
        def block(b, carry):
            these = pl.ds(pl.multiple_of(b * BLOCK, BLOCK), BLOCK)
            for t in range(per_seq):
                for half in range(tile // LANES):
                    rows_in[t * (tile // LANES) + half] = (
                        recv_f[seq * per_seq + t, :, these, half * LANES : (half + 1) * LANES]
                        .astype(F32).reshape(devices * BLOCK, LANES)
                    )
            for pair in range(BLOCK // 2):
                picked = []
                for column in range(2):
                    for t in range(per_seq):
                        at = pl.ds(2 * pair + column, devices, stride=BLOCK)
                        picked.append(
                            jnp.concatenate(
                                [rows_in[t * (tile // LANES) + half, at, :] for half in range(tile // LANES)], axis=1
                            ).astype(BF16)
                        )
                x = jnp.concatenate(picked, axis=0)
                if pair == 0:
                    lone = jnp.logical_and(b == 0, lax.rem(me, per_group) == 0)
                    spread = spread_v[jnp.where(lone, 0, 1)]
                else:
                    spread = spread_v[1]
                u = jnp.dot(spread, x, preferred_element_type=F32)
                cosine, sine = cos_v[...], sin_v[...]
                halves = []
                for half in range(2):
                    real = u[2 * half * first : (2 * half + 1) * first]
                    imag = u[(2 * half + 1) * first : (2 * half + 2) * first]
                    halves.append(
                        jnp.concatenate(
                            [(real * cosine - imag * sine).astype(BF16), (real * sine + imag * cosine).astype(BF16)],
                            axis=1,
                        )
                    )
                turned = jnp.concatenate(halves, axis=0)
                y = lax.dot_general(close_v[...], turned, NT, preferred_element_type=F32)
                for half in range(2):
                    rows_out[pl.ds(2 * pair + half, second, stride=BLOCK), :] = y[:, half * first : (half + 1) * first]

            def leave(there, carry):
                span = second // devices * BLOCK
                out = rows_out[pl.ds(pl.multiple_of(there * span, span), span), :].reshape(-1, BLOCK, LANES)
                for q in range(per_seq):
                    send_r[seq * per_seq + q, there, :, these, :] = out[q * lows : (q + 1) * lows].astype(BF16)
                return carry

            lax.fori_loop(0, devices, leave, 0)
            return carry

        lax.fori_loop(0, channels // BLOCK, block, 0)

    def middle(seq, carry):
        for t in range(per_seq):
            await_all(recv_f, recv_f_sem, seq * per_seq + t)
        transform(seq)
        def gate(at, carry):
            i, n = seq * per_seq + at // (width // WIDE), lax.rem(at, width // WIDE)
            these = wide(n)
            logits = jnp.dot(normed[i], gate_v[:, these], preferred_element_type=F32)
            result[seq, positions(i), these] = jax.nn.sigmoid(logits).astype(BF16)
            return carry

        lax.fori_loop(0, per_seq * (width // WIDE), gate, 0)
        for q in range(per_seq):
            send(send_r, recv_r, send_r_sem, recv_r_sem, seq * per_seq + q)
        return carry

    lax.fori_loop(0, seqs, middle, 0)

    def gather(j):
        await_all(recv_r, recv_r_sem, j)
        left = jnp.concatenate([recv_r[j, :, low].reshape(mixed, LANES) for low in range(lows)], axis=1)
        left_v[...] = lax.dot_general(eye_v[...], left, NT, preferred_element_type=F32).astype(BF16)

    def finish(j, carry):
        gather(j)

        def columns(n, carry):
            at = (j // per_seq, positions(j), wide(n))
            mapped = jnp.dot(left_v[...], out_v[:, wide(n)], preferred_element_type=F32)
            result[at] = (result[at].astype(F32) * mapped).astype(BF16)
            return carry

        lax.fori_loop(0, width // WIDE, columns, 0)
        return carry

    lax.fori_loop(0, tiles - 1, finish, 0)
    gather(tiles - 1)
    for i in range(tiles):
        await_all(send_f, send_f_sem, i)
        await_all(send_r, send_r_sem, i)


def last_kernel(gated, left, out_v, final, stage, sems):
    tile, width = stage.shape
    per_seq = gated.shape[1] // tile
    tiles = sems.shape[0]

    def put(j):
        at = (j // per_seq, pl.ds(j % per_seq * tile, tile))
        return pltpu.make_async_copy(gated.at[at] if j + 1 < tiles else stage, final.at[at], sems.at[j])

    for j in range(tiles - 1):
        put(j).start()

    def columns(n, carry):
        at = pl.ds(pl.multiple_of(n * WIDE, WIDE), WIDE)
        mapped = jnp.dot(left[...], out_v[:, at], preferred_element_type=F32)
        gate = gated[gated.shape[0] - 1, gated.shape[1] - tile :, at].astype(F32)
        stage[:, at] = (gate * mapped).astype(BF16)
        return carry

    lax.fori_loop(0, width // WIDE, columns, 0)
    put(tiles - 1).start()
    for j in range(tiles):
        put(j).wait()


def fused(rows, cols, tokens, norm_gain, mix_weight, gate_weight, out_weight):
    devices = rows * cols
    seqs, here, width = tokens.shape
    length = here * devices
    mixed = mix_weight.shape[1]
    channels = mixed // devices
    first = GROUP_DIM
    second = length // first
    tile = second
    tiles = seqs * here // tile
    lows = tile // first
    normal, lone, cosine, sine, closing = position_tables(devices, length, first)
    constants = [
        jnp.asarray(channel_table().T, BF16),
        jnp.asarray(channel_order(), BF16),
        jnp.asarray(np.eye(tile), BF16),
        jnp.asarray(np.stack([lone.T, normal.T]), BF16),
        jnp.asarray(cosine.T, F32),
        jnp.asarray(sine.T, F32),
        jnp.asarray(closing, BF16),
    ]
    operands = [tokens, norm_gain.reshape(1, width), mix_weight, gate_weight, out_weight, *constants]
    hbm = pl.BlockSpec(memory_space=pl.ANY)
    scratch = [
        pltpu.VMEM((2, tile, width), BF16),
        pltpu.VMEM((tiles, tile, width), BF16),
        pltpu.VMEM(mix_weight.shape, BF16),
        pltpu.VMEM(gate_weight.shape, BF16),
        pltpu.VMEM((1, width), F32),
        *[pltpu.VMEM(constant.shape, constant.dtype) for constant in constants],
        pltpu.VMEM((tiles, devices, channels, tile), BF16),
        pltpu.VMEM((tiles, devices, channels, tile), BF16),
        pltpu.VMEM((tiles, devices, lows, channels, first), BF16),
        pltpu.VMEM((tiles, devices, lows, channels, first), BF16),
        pltpu.VMEM((here // LANES, devices * BLOCK, LANES), F32),
        pltpu.VMEM((second * BLOCK, first), F32),
        pltpu.SemaphoreType.DMA((3 + len(constants),)),
        pltpu.SemaphoreType.DMA((mixed // WIDE,)),
        pltpu.SemaphoreType.DMA((3,)),
        *[pltpu.SemaphoreType.DMA((tiles,)) for _ in range(4)],
        pltpu.SemaphoreType.REGULAR,
    ]
    vmem = pl.BlockSpec(memory_space=pltpu.VMEM)
    made = pl.pallas_call(
        functools.partial(mixer_kernel, rows, cols),
        in_specs=[hbm] * len(operands),
        out_specs=[vmem] * 3,
        out_shape=[
            pltpu.VMEM(tokens.shape, BF16), pltpu.VMEM((tile, mixed), BF16), pltpu.VMEM(out_weight.shape, BF16)
        ],
        scratch_shapes=scratch,
        compiler_params=pltpu.CompilerParams(
            collective_id=0, has_side_effects=True, vmem_limit_bytes=48 * 2**20
        ),
        name="mixer",
    )(*operands)
    return pl.pallas_call(
        last_kernel,
        in_specs=[vmem] * 3,
        out_specs=hbm,
        out_shape=jax.ShapeDtypeStruct(tokens.shape, BF16),
        scratch_shapes=[pltpu.VMEM((tile, width), BF16), pltpu.SemaphoreType.DMA((tiles,))],
        compiler_params=pltpu.CompilerParams(vmem_limit_bytes=4 * 2**20),
        name="last",
    )(*[pltpu.with_memory_space_constraint(array, pltpu.VMEM) for array in made])


def fits(devices, tokens, mix_weight):
    seqs, here, width = tokens.shape
    mixed = mix_weight.shape[1]
    second = here * devices // GROUP_DIM
    return (
        devices % 16 == 0
        and GROUP_DIM % devices == 0
        and mixed % (devices * BLOCK) == 0
        and second % WIDE == 0
        and here % second == 0
        and here // second == GROUP_DIM // devices
        and mixed % WIDE == 0
        and mixed // WIDE >= 4
        and width % WIDE == 0
    )


def local(rows, cols, tokens, norm_gain, mix_weight, gate_weight, out_weight):
    args = (tokens, norm_gain, mix_weight, gate_weight, out_weight)
    if fits(rows * cols, tokens, mix_weight):
        return fused(rows, cols, *args)
    return plain(rows * cols, *args)


def solution(mesh):
    in_specs = (P(None, AXES, None), P(), P(), P(), P())
    body = functools.partial(local, mesh.shape["row"], mesh.shape["col"])
    return jax.shard_map(body, mesh=mesh, in_specs=in_specs, out_specs=P(None, AXES, None), check_vma=False)
```
